512 devices in a mesh: sp: 32 (over z, x), tp: 16 (over y, core).
Axes of the slice: x: 4, y: 8, z: 8, core: 2. Of those that a mesh axis runs over, the one named last changes fastest.
Arguments:
- residual: bfloat16 [16384, 2048], P('sp', 'tp'), may hold values from -64 to 64
- gains: float32 [2, 2, 2048], replicated, may hold values from 0.1 to 1.9
- w_query: bfloat16 [2, 2048, 2048], P(None, None, 'tp'), may hold values from -0.125 to 0.125
- w_key: bfloat16 [2, 2048, 2048], P(None, None, 'tp'), may hold values from -0.125 to 0.125
- w_value: bfloat16 [2, 2048, 2048], P(None, None, 'tp'), may hold values from -0.125 to 0.125
- w_out: bfloat16 [2, 2048, 2048], P(None, None, 'tp'), may hold values from -1 to 1
- rel_bias: float32 [2, 32, 257], P(None, 'tp'), may hold values from -6 to 300
Outputs:
- encoded: bfloat16 [16384, 2048], P('sp', 'tp')
The draws below stay inside these ranges and needn't reach their ends.
All inputs are finite; a program needn't handle non-finite values.
Results may differ from the reference program's by a relative error of at most 0.0058.
Values may be sent and summed in bfloat16 or wider, within the bound.
No kernel may reach another device: no remote copies, remote signals or barrier semaphores. Data moves between devices by JAX's collectives and lax.ppermute only.
A program may use at most 64 MiB of HBM per device.

```python
import jax
import jax.numpy as jnp
from jax import lax

D = 2048
HEADS = 32
HEAD = 64
SEG = 64
LEFT = 8
MAXREL = 128
NREL = 257
LAYERS = 2
TOKENS = 16384


def rough_columns(key, col_count, rise_top):
    spread = jax.random.uniform(key, (col_count,), jnp.float32, -1.0, 1.0)
    ramp = jnp.arange(col_count, dtype=jnp.float32) / col_count
    return rise_top ** ramp * 2.0 ** spread


def draw_residual(key, part):
    key_base, key_rows, key_cols = jax.random.split(jax.random.fold_in(key, 11), 3)
    base = jnp.clip(jax.random.normal(key_base, (TOKENS, D), jnp.float32), -5.0, 5.0)
    row_scale = 0.3 * 10.0 ** jax.random.uniform(key_rows, (TOKENS, 1), jnp.float32)
    col_scale = rough_columns(key_cols, D, 3.0)
    return jnp.clip(base * row_scale * col_scale, -64.0, 64.0).astype(jnp.bfloat16)


def draw_w_out(key, part):
    key_base, key_cols = jax.random.split(jax.random.fold_in(key, 23), 2)
    base = jnp.clip(jax.random.normal(key_base, (LAYERS, D, D), jnp.float32), -5.0, 5.0)
    col_scale = rough_columns(key_cols, D, 3.0)
    scaled = base * col_scale / jnp.sqrt(jnp.float32(D))
    return jnp.clip(scaled, -1.0, 1.0).astype(jnp.bfloat16)


def draw_rel_bias(key, part):
    key_base = jax.random.fold_in(jax.random.fold_in(key, 37), 0)
    base = jnp.clip(jax.random.normal(key_base, (LAYERS, HEADS, NREL), jnp.float32), -6.0, 6.0)
    return base


def block_levels(stream_key, shape, shards, low, largest):
    loudness = 1.0
    for position, parts in shards:
        draws = jax.random.uniform(jax.random.fold_in(jax.random.fold_in(stream_key, 6), position), (parts,), jnp.float32, low / len(shards), largest / len(shards))
        loudness = loudness * jnp.repeat(jnp.exp(draws), shape[position] // parts).reshape((-1,) + (1,) * (len(shape) - 1 - position))
    return loudness


def gaussian(key, dims, scale, most, cuts=(), kind=jnp.bfloat16):
    factor_of = block_levels(key, dims, cuts, -0.22, 0.18) if cuts else 1.0
    values = jax.random.normal(key, dims, jnp.float32) * scale * factor_of
    return jnp.minimum(jnp.maximum(values, -most), most).astype(kind)


def setup_inputs(seed: int = 0) -> dict:
    keys = jax.random.split(jax.random.key(seed), 8)
    return {
        "residual": draw_residual(jax.random.fold_in(keys[7], 71), 0),
        "gains": jnp.clip(1.0 + 0.18 * jax.random.normal(keys[1], (LAYERS, 2, D), jnp.float32), 0.1, 1.9),
        "w_query": gaussian(keys[2], (LAYERS, D, D), D ** -0.5, 0.125, ((2, 16),)),
        "w_key": gaussian(keys[3], (LAYERS, D, D), D ** -0.5, 0.125, ((2, 16),)),
        "w_value": gaussian(keys[4], (LAYERS, D, D), D ** -0.5, 0.125, ((2, 16),)),
        "w_out": draw_w_out(jax.random.fold_in(keys[7], 71), 0),
        "rel_bias": draw_rel_bias(jax.random.fold_in(keys[7], 71), 0),
    }


norm_eps = 1e-06

def norm_rows(values, gain):
    widened = values.astype(jnp.float32)
    inv_rms = lax.rsqrt(lax.optimization_barrier(jnp.mean(widened * widened, axis=1, keepdims=True)) + norm_eps)
    return widened * inv_rms * gain

def attend_all(queries, key_rows, value_rows, bias_table):
    reach_rows = LEFT * SEG
    key_span = reach_rows + 128
    sub_count = queries.shape[0] // 128
    padding = jnp.zeros((reach_rows, key_rows.shape[1]), jnp.bfloat16)
    key_pad = jnp.concatenate([padding, key_rows], axis=0)
    value_pad = jnp.concatenate([padding, value_rows], axis=0)
    row_idx = jnp.arange(128, dtype=jnp.int32)[:, None]
    col_idx = jnp.arange(key_span, dtype=jnp.int32)[None, :]
    distance = reach_rows + row_idx - col_idx
    table_idx = jnp.clip(distance, -MAXREL, MAXREL) + MAXREL
    rel_terms = jnp.take(bias_table, table_idx, axis=1)

    def one_block(block_idx):
        start_row = (block_idx * 128).astype(jnp.int32)
        query_sub = lax.dynamic_slice_in_dim(queries, start_row, 128, 0).reshape(128, HEADS, HEAD).astype(jnp.float32)
        key_sub = lax.dynamic_slice_in_dim(key_pad, start_row, key_span, 0).reshape(key_span, HEADS, HEAD).astype(jnp.float32)
        value_sub = lax.dynamic_slice_in_dim(value_pad, start_row, key_span, 0).reshape(key_span, HEADS, HEAD).astype(jnp.float32)
        scores = jnp.einsum('qhd,khd->hqk', query_sub, key_sub) * HEAD ** (-0.5) + rel_terms
        query_pos = start_row + row_idx
        key_pos = start_row - reach_rows + col_idx
        seg_gap = jnp.floor_divide(query_pos, SEG) - jnp.floor_divide(key_pos, SEG)
        allowed = (key_pos >= 0) & (seg_gap >= 0) & (seg_gap <= LEFT)
        scores = jnp.where(allowed[None], scores, -jnp.inf)
        row_max = lax.optimization_barrier(jnp.max(scores, axis=2, keepdims=True))
        weights_raw = jnp.exp(scores - row_max)
        prob_bf = (weights_raw / lax.optimization_barrier(jnp.sum(weights_raw, axis=2, keepdims=True))).astype(jnp.bfloat16)
        result = jnp.einsum('hqk,khd->qhd', prob_bf.astype(jnp.float32), value_sub)
        return result.astype(jnp.bfloat16).reshape(128, HEADS * HEAD)
    blocks = lax.map(one_block, jnp.arange(sub_count, dtype=jnp.int32))
    return blocks.reshape(queries.shape[0], HEADS * HEAD)

def reference(residual, gains, w_query, w_key, w_value, w_out, rel_bias):
    stream = residual
    for layer_idx in range(LAYERS):
        normed = norm_rows(stream, gains[layer_idx, 0]).astype(jnp.bfloat16)
        queries = jnp.dot(normed, w_query[layer_idx], preferred_element_type=jnp.float32).astype(jnp.bfloat16)
        key_rows = jnp.dot(normed, w_key[layer_idx], preferred_element_type=jnp.float32).astype(jnp.bfloat16)
        value_rows = jnp.dot(normed, w_value[layer_idx], preferred_element_type=jnp.float32).astype(jnp.bfloat16)
        attended = attend_all(queries, key_rows, value_rows, rel_bias[layer_idx])
        branch = jnp.dot(attended, w_out[layer_idx], preferred_element_type=jnp.float32)
        stream = (stream.astype(jnp.float32) + norm_rows(branch, gains[layer_idx, 1])).astype(jnp.bfloat16)
    return stream
```

```python
import functools

import jax
import jax.numpy as jnp
from jax import lax
from jax.experimental import pallas as pl
from jax.experimental.pallas import tpu as pltpu
from jax.sharding import Mesh
from jax.sharding import PartitionSpec as P

D = 2048
HEAD = 64
BLK = 128
NB = 16
EPS = 1e-06
NEG = -1e30
VMEM = pl.BlockSpec(memory_space=pltpu.VMEM)
SMEM = pl.BlockSpec(memory_space=pltpu.SMEM)


def params(mib):
    return pltpu.CompilerParams(vmem_limit_bytes=mib * 1024 * 1024)


def core_pairs(step):
    pairs = []
    for y in range(8):
        for c in range(2):
            target = (y + (step if c == 0 else -step)) % 8
            pairs.append((2 * y + c, 2 * target + c))
    return pairs


def gather_blocks(x):
    core = lax.axis_index("c")
    own = lax.all_gather(x, "c", axis=0)
    one = lax.ppermute(own, ("y", "c"), core_pairs(1))
    two = lax.ppermute(own, ("y", "c"), core_pairs(2))
    three = lax.ppermute(two, ("y", "c"), core_pairs(1))
    half = lax.dynamic_index_in_dim(two, core, 0, keepdims=True)
    four = lax.ppermute(half, ("y", "c"), core_pairs(2))
    received = jnp.concatenate([one, two, three, four], axis=0)
    other = lax.ppermute(received, "c", [(0, 1), (1, 0)])
    return own, received, other


def block_ids():
    y = lax.axis_index("y")
    c = lax.axis_index("c")
    sign = 1 - 2 * c
    near = [(y - sign * d) % 8 for d in (1, 2, 3)]
    far = [(y + sign * d) % 8 for d in (1, 2, 3)]
    across = (y + 4) % 8
    ids = [2 * y, 2 * y + 1]
    for chip in near:
        ids += [2 * chip, 2 * chip + 1]
    ids.append(2 * across + c)
    for chip in far:
        ids += [2 * chip, 2 * chip + 1]
    ids.append(2 * across + 1 - c)
    return jnp.stack(ids).astype(jnp.int32)


def part(refs, k):
    own, received, other = refs
    if k < 2:
        return own, k
    if k < 9:
        return received, k - 2
    return other, k - 9


def qkv_tail(ids, xs, total, gain, rows, norm):
    inv = lax.rsqrt(jnp.sum(total, axis=1, keepdims=True) / D + EPS)
    for k in range(NB):
        t = ids[k]
        col = pl.multiple_of(t * BLK, BLK)
        norm[rows, pl.ds(col, BLK)] = (
            xs(k) * inv * gain[pl.ds(t, 1), :]
        ).astype(jnp.bfloat16)


def project(norm, wq, wk, wv, q_out, kv_out):
    full = norm[...]
    kv_out[:, :BLK] = jnp.dot(full, wk[...], preferred_element_type=jnp.float32).astype(jnp.bfloat16)
    kv_out[:, BLK:] = jnp.dot(full, wv[...], preferred_element_type=jnp.float32).astype(jnp.bfloat16)
    q = jnp.dot(full, wq[...], preferred_element_type=jnp.float32)
    q_out[...] = (q * HEAD ** (-0.5)).astype(jnp.bfloat16)


def first_kernel(ids, own, received, other, gain, wq, wk, wv, q_out, kv_out, norm):
    refs = (own, received, other)

    def tile(i, carry):
        rows = pl.ds(pl.multiple_of(i * 64, 64), 64)

        def load(k):
            ref, j = part(refs, k)
            return ref[j, rows, :].astype(jnp.float32)

        total = jnp.zeros((64, BLK), jnp.float32)
        for k in range(NB):
            x = load(k)
            total += x * x
        qkv_tail(ids, load, total, gain, rows, norm)
        return carry

    lax.fori_loop(0, own.shape[1] // 64, tile, 0)
    project(norm, wq, wk, wv, q_out, kv_out)


def next_kernel(
    ids, mine, own, received, other, b_own, b_received, b_other, gain_post, gain, wq, wk, wv,
    q_out, kv_out, stream_out, norm, stream,
):
    refs = (own, received, other)
    b_refs = (b_own, b_received, b_other)

    def tile(i, carry):
        rows = pl.ds(pl.multiple_of(i * 64, 64), 64)

        def load(group, k):
            ref, j = part(group, k)
            return ref[j, rows, :].astype(jnp.float32)

        total = jnp.zeros((64, BLK), jnp.float32)
        for k in range(NB):
            x = load(b_refs, k)
            total += x * x
        inv_post = lax.rsqrt(jnp.sum(total, axis=1, keepdims=True) / D + EPS)
        total = jnp.zeros((64, BLK), jnp.float32)
        for k in range(NB):
            x = load(refs, k) + load(b_refs, k) * inv_post * gain_post[pl.ds(ids[k], 1), :]
            x = x.astype(jnp.bfloat16)
            stream[k, rows, :] = x
            x = x.astype(jnp.float32)
            total += x * x
        qkv_tail(ids, lambda k: stream[k, rows, :].astype(jnp.float32), total, gain, rows, norm)
        stream_out[rows, :] = stream[mine[0], rows, :]
        return carry

    lax.fori_loop(0, own.shape[1] // 64, tile, 0)
    project(norm, wq, wk, wv, q_out, kv_out)


def attend_kernel(layer, first, q, kv, kv_prev, bias, out):
    lane = lax.broadcasted_iota(jnp.int32, (BLK, BLK), 1)
    row = lax.broadcasted_iota(jnp.int32, (BLK, BLK), 0)
    hidden = jnp.where(first[0] == 1, NEG, 0.0)
    tables = []
    for h in range(2):
        low = bias[layer, h : h + 1, 0:BLK]
        high = bias[layer, h : h + 1, BLK : 2 * BLK]
        last = bias[layer, h : h + 1, 2 * BLK : 2 * BLK + 1]
        last_row = jnp.broadcast_to(last, (1, BLK))
        shape = (BLK, 2 * BLK)
        diag = jnp.broadcast_to(jnp.concatenate([high, low], axis=1), shape)
        diag = pltpu.roll(diag, 0, 1, stride=1, stride_axis=0)[:, :BLK].T
        near = jnp.broadcast_to(jnp.concatenate([last_row, high], axis=1), shape)
        near = pltpu.roll(near, 0, 1, stride=1, stride_axis=0)[:, :BLK].T
        diag = jnp.where((lane >= 64) & (row < 64), NEG, diag)
        full_last = jnp.broadcast_to(last, (BLK, BLK))
        edge = jnp.where((lane < 64) & (row >= 64), NEG, full_last)
        tables.append((diag, near, full_last, edge))
    for i in range(4):
        rows = slice(i * BLK, (i + 1) * BLK)
        results = []
        for h in range(2):
            diag, near, full_last, edge = tables[h]
            qh = q[rows, :]
            qh = jnp.where((lane < HEAD) == (h == 0), qh, jnp.zeros_like(qh))
            dims = (((1,), (1,)), ((), ()))
            left = lax.dot_general(
                qh, kv_prev[i * BLK :, :BLK], dims, preferred_element_type=jnp.float32
            )
            right = lax.dot_general(
                qh, kv[: (i + 1) * BLK, :BLK], dims, preferred_element_type=jnp.float32
            )
            scores = []
            for j in range(5):
                gap = 4 - j
                block = i + j
                if block < 4:
                    piece = left[:, j * BLK : (j + 1) * BLK] + hidden
                else:
                    piece = right[:, (block - 4) * BLK : (block - 3) * BLK]
                term = diag if gap == 0 else near if gap == 1 else edge if gap == 4 else full_last
                scores.append(piece + term)
            top = functools.reduce(jnp.maximum, scores)
            top = jnp.max(top, axis=1, keepdims=True)
            weights = [jnp.exp(s - top) for s in scores]
            norm = jnp.sum(functools.reduce(jnp.add, weights), axis=1, keepdims=True)
            inv = 1.0 / norm
            probs = [(w * inv).astype(jnp.bfloat16) for w in weights]
            split = 4 - i
            acc = jnp.dot(
                jnp.concatenate(probs[:split], axis=1),
                kv_prev[i * BLK :, BLK:],
                preferred_element_type=jnp.float32,
            )
            acc += jnp.dot(
                jnp.concatenate(probs[split:], axis=1),
                kv[: (i + 1) * BLK, BLK:],
                preferred_element_type=jnp.float32,
            )
            results.append(acc)
        out[rows, :] = jnp.where(lane < HEAD, results[0], results[1]).astype(jnp.bfloat16)


def branch_of(ids, refs, w, acc):
    acc[...] = jnp.zeros_like(acc)
    for k in (0, 2, 4, 6, 9, 11, 13):
        ref, j = part(refs, k)
        pair = jnp.concatenate([ref[j], ref[j + 1]], axis=1)
        rows = pl.ds(pl.multiple_of(ids[k] * BLK, 2 * BLK), 2 * BLK)
        acc[...] += jnp.dot(pair, w[rows, :], preferred_element_type=jnp.float32)
    for k in (8, 15):
        ref, j = part(refs, k)
        rows = pl.ds(pl.multiple_of(ids[k] * BLK, BLK), BLK)
        acc[...] += jnp.dot(ref[j], w[rows, :], preferred_element_type=jnp.float32)


def out_kernel(ids, own, received, other, w, out, acc):
    branch_of(ids, (own, received, other), w, acc)
    out[...] = acc[...].astype(jnp.bfloat16)


def last_kernel(ids, own, received, other, w, out, squares):
    branch_of(ids, (own, received, other), w, out)
    for i in range(4):
        x = out[i * BLK : (i + 1) * BLK, :]
        squares[i : i + 1, :] = jnp.sum((x * x).T, axis=0, keepdims=True)


def finish_kernel(squares, branch, stream, gain, out):
    total = jnp.sum(squares[...], axis=0)
    inv = lax.rsqrt(total / D + EPS)
    for i in range(4):
        rows = slice(i * BLK, (i + 1) * BLK)
        scale = jnp.broadcast_to(inv[i : i + 1, :], (BLK, BLK)).T
        x = stream[rows, :].astype(jnp.float32)
        out[rows, :] = (x + branch[rows, :] * scale * gain[...]).astype(jnp.bfloat16)


def call(kernel, ins, outs, scratch, mib, flops, args):
    size = sum(a.size * a.dtype.itemsize for a in args)
    return pl.pallas_call(
        kernel,
        out_shape=outs,
        in_specs=ins,
        out_specs=jax.tree.map(lambda _: VMEM, outs),
        scratch_shapes=scratch,
        compiler_params=params(mib),
        cost_estimate=pl.CostEstimate(flops=flops, bytes_accessed=size, transcendentals=0),
    )(*args)


def on_device(residual, gains, w_query, w_key, w_value, w_out, rel_bias):
    tokens = residual.shape[0]
    half = jnp.bfloat16
    ids = block_ids()
    core = lax.axis_index("c")
    mine = core.reshape(1).astype(jnp.int32)
    first = (lax.axis_index("sp") == 0).reshape(1).astype(jnp.int32)
    gain_rows = gains.reshape(2, 2, NB, BLK)
    own_gain = lax.dynamic_slice_in_dim(gain_rows[1, 1], lax.axis_index(("y", "c")), 1, 0)
    block = jax.ShapeDtypeStruct((tokens, BLK), half)
    pair = jax.ShapeDtypeStruct((tokens, 2 * BLK), half)
    wide = jax.ShapeDtypeStruct((tokens, BLK), jnp.float32)
    norm = pltpu.VMEM((tokens, D), half)
    flow = lax.axis_size("sp")
    shift = [(i, i + 1) for i in range(flow - 1)]

    def attention(layer, q, kv):
        previous = lax.ppermute(kv, "sp", shift)
        return call(
            functools.partial(attend_kernel, layer), [SMEM] + [VMEM] * 4, block, [], 8,
            10**9, (first, q, kv, previous, rel_bias),
        )

    stream = gather_blocks(residual)
    q, kv = call(
        first_kernel, [SMEM] + [VMEM] * 7, (block, pair), [norm], 16, 2 * 10**9,
        (ids, *stream, gain_rows[0, 0], w_query[0], w_key[0], w_value[0]),
    )
    attended = gather_blocks(attention(0, q, kv))
    branch = call(
        out_kernel, [SMEM] + [VMEM] * 4, block, [pltpu.VMEM((tokens, BLK), jnp.float32)], 8,
        10**9, (ids, *attended, w_out[0]),
    )
    branch = gather_blocks(branch)
    q, kv, carried = call(
        next_kernel, [SMEM] * 2 + [VMEM] * 11, (block, pair, block),
        [norm, pltpu.VMEM((NB, tokens, BLK), half)], 20, 2 * 10**9,
        (ids, mine, *stream, *branch, gain_rows[0, 1], gain_rows[1, 0],
         w_query[1], w_key[1], w_value[1]),
    )
    attended = gather_blocks(attention(1, q, kv))
    branch, squares = call(
        last_kernel, [SMEM] + [VMEM] * 4,
        (wide, jax.ShapeDtypeStruct((tokens // BLK, BLK), jnp.float32)), [], 8, 10**9,
        (ids, *attended, w_out[1]),
    )
    copies = jnp.broadcast_to(squares, (NB, *squares.shape))
    everything = lax.all_to_all(copies, ("y", "c"), split_axis=0, concat_axis=0, tiled=True)
    return call(
        finish_kernel, [VMEM] * 4, block, [], 8, 10**7, (everything, branch, carried, own_gain)
    )


def solution(mesh):
    finer = Mesh(mesh.devices.reshape(mesh.shape["sp"], 8, 2), ("sp", "y", "c"))
    tp = ("y", "c")
    in_specs = (
        P("sp", tp),
        P(),
        P(None, None, tp),
        P(None, None, tp),
        P(None, None, tp),
        P(None, None, tp),
        P(None, tp, None),
    )
    return jax.shard_map(
        on_device, mesh=finer, in_specs=in_specs, out_specs=P("sp", tp), check_vma=False
    )
```

```python
import functools

import jax
import jax.numpy as jnp
from jax import lax
from jax.experimental import pallas as pl
from jax.experimental.pallas import tpu as pltpu
from jax.sharding import Mesh
from jax.sharding import PartitionSpec as P


D = 2048
HEAD = 64
BLK = 128
NB = 16
EPS = 1e-06
BIG = 60
NEG = -1e30
VMEM = pl.BlockSpec(memory_space=pltpu.VMEM)
SMEM = pl.BlockSpec(memory_space=pltpu.SMEM)
HBM = pl.BlockSpec(memory_space=pltpu.HBM)


def params(mib):
    return pltpu.CompilerParams(vmem_limit_bytes=mib * 1024 * 1024)


def core_pairs(step):
    pairs = []
    for y in range(8):
        for c in range(2):
            target = (y + (step if c == 0 else -step)) % 8
            pairs.append((2 * y + c, 2 * target + c))
    return pairs


def gather_blocks(x):
    core = lax.axis_index("c")

    own = lax.all_gather(x, "c", axis=0)
    two = lax.ppermute(own, ("y", "c"), core_pairs(2))
    one = lax.ppermute(own, ("y", "c"), core_pairs(1))
    half = lax.dynamic_index_in_dim(two, core, 0, keepdims=True)
    three = lax.ppermute(two, ("y", "c"), core_pairs(1))
    four = lax.ppermute(half, ("y", "c"), core_pairs(2))
    received = jnp.concatenate([one, two, three, four], axis=0)
    other = lax.ppermute(received, "c", [(0, 1), (1, 0)])
    return own, received, other


def block_ids():
    y = lax.axis_index("y")
    c = lax.axis_index("c")
    sign = 1 - 2 * c
    near = [(y - sign * d) % 8 for d in (1, 2, 3)]
    far = [(y + sign * d) % 8 for d in (1, 2, 3)]
    across = (y + 4) % 8
    ids = [2 * y, 2 * y + 1]
    for chip in near:
        ids += [2 * chip, 2 * chip + 1]
    ids.append(2 * across + c)
    for chip in far:
        ids += [2 * chip, 2 * chip + 1]
    ids.append(2 * across + 1 - c)
    return jnp.stack(ids).astype(jnp.int32)


def part(refs, k):
    own, received, other = refs
    if k < 2:
        return own, k
    if k < 9:
        return received, k - 2
    return other, k - 9


def scale_kernel(layer, count, ids, gain, *refs):
    weights, (out, *held, sems) = refs[:count], refs[count:]
    copies = [
        pltpu.make_async_copy(w.at[layer], dst, sems.at[n])
        for n, (w, dst) in enumerate(zip(weights, held))
    ]
    for copy in copies:
        copy.start()
    for copy in copies:
        copy.wait()
    for k in range(NB):
        t = ids[k]
        rows = pl.ds(pl.multiple_of(t * BLK, BLK), BLK)
        factor = jnp.broadcast_to(gain_row(gain, layer, 0, t), (BLK, BLK)).T
        for n, w in enumerate(held):
            scaled = w[rows, :].astype(jnp.float32) * factor
            out[k, :, n * BLK : (n + 1) * BLK] = scaled.astype(jnp.bfloat16)


def gain_row(gain, layer, kind, t):
    return gain[layer, kind : kind + 1, pl.ds(pl.multiple_of(t * BLK, BLK), BLK)]


def product(blocks, w):
    left = jnp.concatenate(blocks, axis=1)
    return jnp.dot(left, w[...].reshape(D, w.shape[2]), preferred_element_type=jnp.float32)


def blocks_of(refs):
    if len(refs) == 1:
        return [refs[0][k] for k in range(NB)]
    pairs = [part(refs, k) for k in range(NB)]
    return [ref[j] for ref, j in pairs]


def wide_inverse(total):
    inv = lax.rsqrt(jnp.sum(total, axis=1, keepdims=True) / D + EPS)
    return jnp.broadcast_to(inv, total.shape)


def first_kernel(own, received, other, w, kv_out, inv_out):
    refs = (own, received, other)

    def tile(i, carry):
        rows = pl.ds(pl.multiple_of(i * 64, 64), 64)
        total = jnp.zeros((64, BLK), jnp.float32)
        for k in range(NB):
            ref, j = part(refs, k)
            x = ref[j, rows, :].astype(jnp.float32)
            total += x * x
        inv_out[rows, :] = wide_inverse(total)
        return carry

    lax.fori_loop(0, own.shape[1] // 64, tile, 0)
    inv = inv_out[...]
    kv = product(blocks_of(refs), w)
    kv_out[...] = (kv * jnp.concatenate([inv, inv], axis=1)).astype(jnp.bfloat16)


def next_kernel(
    ids, mine, own, received, other, b_own, b_received, b_other, gain, w,
    kv_out, inv_out, stream, carried,
):
    refs = (own, received, other)
    b_refs = (b_own, b_received, b_other)

    def tile(i, carry):
        rows = pl.ds(pl.multiple_of(i * 64, 64), 64)

        def load(group, k):
            ref, j = part(group, k)
            return ref[j, rows, :].astype(jnp.float32)

        total = jnp.zeros((64, BLK), jnp.float32)
        for k in range(NB):
            x = load(b_refs, k)
            total += x * x
        inv_post = wide_inverse(total)
        total = jnp.zeros((64, BLK), jnp.float32)
        for k in range(NB):
            x = load(refs, k) + load(b_refs, k) * inv_post * gain_row(gain, 0, 1, ids[k])
            x = x.astype(jnp.bfloat16)
            stream[k, rows, :] = x
            x = x.astype(jnp.float32)
            total += x * x
        inv_out[rows, :] = wide_inverse(total)
        carried[rows, :] = stream[mine[0], rows, :]
        return carry

    lax.fori_loop(0, own.shape[1] // 64, tile, 0)
    inv = inv_out[...]
    kv = product(blocks_of((stream,)), w)
    kv_out[...] = (kv * jnp.concatenate([inv, inv], axis=1)).astype(jnp.bfloat16)


def grids():
    lane = lax.broadcasted_iota(jnp.int32, (BLK, BLK), 1)
    row = lax.broadcasted_iota(jnp.int32, (BLK, BLK), 0)
    return lane, row


def split_bias(bias, layer, h):
    low = bias[layer, h : h + 1, 0:BLK]
    high = bias[layer, h : h + 1, BLK : 2 * BLK]
    last = bias[layer, h : h + 1, 2 * BLK : 2 * BLK + 1]
    return low, high, last


def skewed(left, right):
    full = jnp.broadcast_to(jnp.concatenate([left, right], axis=1), (BLK, 2 * BLK))
    return pltpu.roll(full, 0, 1, stride=1, stride_axis=0)[:, :BLK].T


def head_scores(qh, keys):
    dims = (((1,), (1,)), ((), ()))
    return lax.dot_general(qh, keys, dims, preferred_element_type=jnp.float32)


def local_kernel(layer, x_count, *refs):
    xs, rest = refs[:x_count], refs[x_count:]
    w, inv, kv, bias, q_out, acc_out, top_out, sum_out, near_out = rest
    q = product(blocks_of(xs), w)
    q_out[...] = (q * inv[...] * HEAD ** (-0.5)).astype(jnp.bfloat16)
    lane, row = grids()
    tables = []
    for h in range(2):
        low, high, last = split_bias(bias, layer, h)
        last_row = jnp.broadcast_to(last, (1, BLK))
        diag = jnp.where((lane >= 64) & (row < 64), NEG, skewed(high, low))
        near_out[h] = skewed(last_row, high)
        tables.append((diag, near_out[h], jnp.broadcast_to(last, (BLK, BLK))))
    for i in range(4):
        rows = slice(i * BLK, (i + 1) * BLK)
        found = []
        for h in range(2):
            qh = q_out[rows, :]
            qh = jnp.where((lane < HEAD) == (h == 0), qh, jnp.zeros_like(qh))
            raw = head_scores(qh, kv[: (i + 1) * BLK, :BLK])
            scores = [
                raw[:, j * BLK : (j + 1) * BLK] + tables[h][min(i - j, 2)] for j in range(i + 1)
            ]
            top = jnp.max(functools.reduce(jnp.maximum, scores), axis=1, keepdims=True)
            weights = [jnp.exp(s - top) for s in scores]
            norm = jnp.sum(functools.reduce(jnp.add, weights), axis=1, keepdims=True)
            probs = jnp.concatenate([x.astype(jnp.bfloat16) for x in weights], axis=1)
            acc = jnp.dot(probs, kv[: (i + 1) * BLK, BLK:], preferred_element_type=jnp.float32)
            found.append((acc, top, norm))
        for n, out in enumerate((acc_out, top_out, sum_out)):
            out[rows, :] = jnp.where(lane < HEAD, found[0][n], found[1][n])


def merge_kernel(layer, first, q, kv, acc, top, total, nears, bias, out):
    lane, row = grids()
    hidden = jnp.where(first[0] == 1, NEG, 0.0)
    tables = []
    for h in range(2):
        last = split_bias(bias, layer, h)[2]
        full = jnp.broadcast_to(last, (BLK, BLK)) + hidden
        edge = jnp.where((lane < 64) & (row >= 64), NEG, full)
        tables.append((nears[h] + hidden, full, edge))
    for i in range(4):
        rows = slice(i * BLK, (i + 1) * BLK)
        found = []
        for h in range(2):
            near, full, edge = tables[h]
            qh = q[rows, :]
            qh = jnp.where((lane < HEAD) == (h == 0), qh, jnp.zeros_like(qh))
            raw = head_scores(qh, kv[i * BLK :, :BLK])
            scores = []
            for j in range(4 - i):
                term = edge if j == 0 else near if j == 3 else full
                scores.append(raw[:, j * BLK : (j + 1) * BLK] + term)
            old = top[rows, h * HEAD : h * HEAD + 1]
            peak = jnp.max(functools.reduce(jnp.maximum, scores), axis=1, keepdims=True)
            peak = jnp.maximum(peak, old)
            weights = [jnp.exp(s - peak) for s in scores]
            norm = jnp.sum(functools.reduce(jnp.add, weights), axis=1, keepdims=True)
            probs = jnp.concatenate([x.astype(jnp.bfloat16) for x in weights], axis=1)
            part_acc = jnp.dot(probs, kv[i * BLK :, BLK:], preferred_element_type=jnp.float32)
            found.append((part_acc, jnp.exp(old - peak), norm))
        more, fade, norm = (jnp.where(lane < HEAD, found[0][n], found[1][n]) for n in range(3))
        result = (acc[rows, :] * fade + more) / (total[rows, :] * fade + norm)
        out[rows, :] = result.astype(jnp.bfloat16)


def branch_of(ids, refs, w, acc):
    acc[...] = jnp.zeros_like(acc)
    for k in (0, 2, 4, 6, 9, 11, 13):
        ref, j = part(refs, k)
        pair = jnp.concatenate([ref[j], ref[j + 1]], axis=1)
        rows = pl.ds(pl.multiple_of(ids[k] * BLK, 2 * BLK), 2 * BLK)
        acc[...] += jnp.dot(pair, w[rows, :], preferred_element_type=jnp.float32)
    for k in (8, 15):
        ref, j = part(refs, k)
        rows = pl.ds(pl.multiple_of(ids[k] * BLK, BLK), BLK)
        acc[...] += jnp.dot(ref[j], w[rows, :], preferred_element_type=jnp.float32)


def out_kernel(ids, own, received, other, w, out, acc):
    branch_of(ids, (own, received, other), w, acc)
    out[...] = acc[...].astype(jnp.bfloat16)


def last_kernel(ids, own, received, other, w, out, squares):
    branch_of(ids, (own, received, other), w, out)
    for i in range(4):
        x = out[i * BLK : (i + 1) * BLK, :]
        sums = jnp.sum((x * x).T, axis=0, keepdims=True)
        for n in range(NB):
            squares[n, i : i + 1, :] = sums


def finish_kernel(ids, mine, squares, branch, stream, gain, out):
    total = jnp.sum(squares[...], axis=0)
    inv = lax.rsqrt(total / D + EPS)
    own_gain = gain_row(gain, 1, 1, ids[mine[0]])
    for i in range(4):
        rows = slice(i * BLK, (i + 1) * BLK)
        scale = jnp.broadcast_to(inv[i : i + 1, :], (BLK, BLK)).T
        x = stream[rows, :].astype(jnp.float32)
        out[rows, :] = (x + branch[rows, :] * scale * own_gain).astype(jnp.bfloat16)


def call(kernel, ins, outs, scratch, mib, flops, args):
    size = sum(a.size * a.dtype.itemsize for a in args)
    return pl.pallas_call(
        kernel,
        out_shape=outs,
        in_specs=ins,
        out_specs=jax.tree.map(lambda _: VMEM, outs),
        scratch_shapes=scratch,
        compiler_params=params(mib),
        cost_estimate=pl.CostEstimate(flops=flops, bytes_accessed=size, transcendentals=0),
    )(*args)


def on_device(residual, gains, w_query, w_key, w_value, w_out, rel_bias):
    tokens = residual.shape[0]
    half = jnp.bfloat16
    ids = block_ids()
    core = lax.axis_index("c")
    mine = core.reshape(1).astype(jnp.int32)
    first = (lax.axis_index("sp") == 0).reshape(1).astype(jnp.int32)
    block = jax.ShapeDtypeStruct((tokens, BLK), half)
    pair = jax.ShapeDtypeStruct((tokens, 2 * BLK), half)
    wide = jax.ShapeDtypeStruct((tokens, BLK), jnp.float32)
    stack = jax.ShapeDtypeStruct((NB, tokens, BLK), half)
    tiles = jax.ShapeDtypeStruct((2, BLK, BLK), jnp.float32)
    flow = lax.axis_size("sp")
    shift = [(i, i + 1) for i in range(flow - 1)]

    def scaled(layer, weights, mib):
        count = len(weights)
        shape = jax.ShapeDtypeStruct((NB, BLK, count * BLK), half)
        scratch = [pltpu.VMEM((D, BLK), half)] * count + [pltpu.SemaphoreType.DMA((count,))]
        return call(
            functools.partial(scale_kernel, layer, count), [SMEM, VMEM] + [HBM] * count,
            shape, scratch, mib, 10**9, (ids, gains, *weights),
        )

    def attention(layer, xs, wq, kv, inv):
        previous = lax.ppermute(kv, "sp", shift)
        local = call(
            functools.partial(local_kernel, layer, len(xs)), [VMEM] * (len(xs) + 4),
            (block, wide, wide, wide, tiles), [], 4, 2 * 10**9, (*xs, wq, inv, kv, rel_bias),
        )
        return call(
            functools.partial(merge_kernel, layer), [SMEM] + [VMEM] * 7, block, [], 4,
            10**9, (first, local[0], previous, *local[1:], rel_bias),
        )

    wkv = scaled(0, (w_key, w_value), BIG)
    wq = scaled(0, (w_query,), 4)
    stream = gather_blocks(residual)
    kv, inv = call(
        first_kernel, [VMEM] * 4, (pair, wide), [], 4, 2 * 10**9, (*stream, wkv),
    )
    attended = gather_blocks(attention(0, stream, wq, kv, inv))
    branch = call(
        out_kernel, [SMEM] + [VMEM] * 4, block, [pltpu.VMEM((tokens, BLK), jnp.float32)], 4,
        10**9, (ids, *attended, w_out[0]),
    )
    branch = gather_blocks(branch)
    wkv = scaled(1, (w_key, w_value), 4)
    wq = scaled(1, (w_query,), 4)
    kv, inv, full, carried = call(
        next_kernel, [SMEM] * 2 + [VMEM] * 8, (pair, wide, stack, block), [], 4, 2 * 10**9,
        (ids, mine, *stream, *branch, gains, wkv),
    )
    attended = gather_blocks(attention(1, (full,), wq, kv, inv))
    branch, squares = call(
        last_kernel, [SMEM] + [VMEM] * 4,
        (wide, jax.ShapeDtypeStruct((NB, tokens // BLK, BLK), jnp.float32)), [], 4, 10**9,
        (ids, *attended, w_out[1]),
    )
    everything = lax.all_to_all(squares, ("y", "c"), split_axis=0, concat_axis=0, tiled=True)
    return call(
        finish_kernel, [SMEM] * 2 + [VMEM] * 4, block, [], 4, 10**7,
        (ids, mine, everything, branch, carried, gains),
    )


def solution(mesh):
    finer = Mesh(mesh.devices.reshape(mesh.shape["sp"], 8, 2), ("sp", "y", "c"))
    tp = ("y", "c")
    in_specs = (
        P("sp", tp),
        P(),
        P(None, None, tp),
        P(None, None, tp),
        P(None, None, tp),
        P(None, None, tp),
        P(None, tp, None),
    )

    return jax.shard_map(
        on_device, mesh=finer, in_specs=in_specs, out_specs=P("sp", tp), check_vma=False
    )
```

```python
import functools

import jax
import jax.numpy as jnp
from jax import lax
from jax.experimental import pallas as pl
from jax.experimental.pallas import tpu as pltpu
from jax.sharding import Mesh
from jax.sharding import PartitionSpec as P


D = 2048
HEAD = 64
BLK = 128
NB = 16
EPS = 1e-06
BIG = 60
CUTS = 4
NEG = -1e30
VMEM = pl.BlockSpec(memory_space=pltpu.VMEM)
SMEM = pl.BlockSpec(memory_space=pltpu.SMEM)
HBM = pl.BlockSpec(memory_space=pltpu.HBM)


def params(mib):
    return pltpu.CompilerParams(vmem_limit_bytes=mib * 1024 * 1024)


def core_pairs(step):
    pairs = []
    for y in range(8):
        for c in range(2):
            target = (y + (step if c == 0 else -step)) % 8
            pairs.append((2 * y + c, 2 * target + c))
    return pairs


def gather_blocks(x):
    core = lax.axis_index("c")

    own = lax.all_gather(x, "c", axis=0)
    two = lax.ppermute(own, ("y", "c"), core_pairs(2))
    one = lax.ppermute(own, ("y", "c"), core_pairs(1))
    half = lax.dynamic_index_in_dim(two, core, 0, keepdims=True)
    three = lax.ppermute(two, ("y", "c"), core_pairs(1))
    four = lax.ppermute(half, ("y", "c"), core_pairs(2))
    received = jnp.concatenate([one, two, three, four], axis=0)
    other = lax.ppermute(received, "c", [(0, 1), (1, 0)])
    return own, received, other


def block_ids(place):
    y, c = place[0] // 2, place[0] % 2
    sign = 1 - 2 * c
    across = 2 * ((y + 4) % 8)
    ids = [2 * y, 2 * y + 1]
    for way, last in ((-sign, c), (sign, 1 - c)):
        for d in (1, 2, 3):
            chip = (y + way * d + 8) % 8
            ids += [2 * chip, 2 * chip + 1]
        ids.append(across + last)
    return ids


def part(refs, k):
    own, received, other = refs
    if k < 2:
        return own, k
    if k < 9:
        return received, k - 2
    return other, k - 9


def scale_kernel(layer, count, place, gain, *refs):
    weights, (out, *held, sems) = refs[:count], refs[count:]
    ids = block_ids(place)
    copies = []
    for n, (w, dst) in enumerate(zip(weights, held)):
        for m in range(CUTS):
            rows = pl.ds(m * (D // CUTS), D // CUTS)
            copies.append(
                pltpu.make_async_copy(w.at[layer, rows, :], dst.at[rows, :], sems.at[n, m])
            )
    for copy in copies:
        copy.start()
    for copy in copies:
        copy.wait()
    for k in range(NB):
        t = ids[k]
        rows = pl.ds(pl.multiple_of(t * BLK, BLK), BLK)
        factor = jnp.broadcast_to(gain_row(gain, layer, 0, t), (BLK, BLK)).T
        for n, w in enumerate(held):
            scaled = w[rows, :].astype(jnp.float32) * factor
            out[k, :, n * BLK : (n + 1) * BLK] = scaled.astype(jnp.bfloat16)


def gain_row(gain, layer, kind, t):
    return gain[layer, kind : kind + 1, pl.ds(pl.multiple_of(t * BLK, BLK), BLK)]


def product(blocks, weights):
    left = jnp.concatenate(blocks, axis=1)
    right = jnp.concatenate(
        [jnp.concatenate([w[k] for w in weights], axis=1) for k in range(len(blocks))], axis=0
    )
    return jnp.dot(left, right, preferred_element_type=jnp.float32)


def blocks_of(refs):
    return [ref[k] for ref in refs for k in range(ref.shape[0])]


def row_squares(refs, rows):
    total = jnp.zeros((rows.size, BLK), jnp.float32)
    for ref in refs:
        for k in range(ref.shape[0]):
            x = ref[k, rows, :].astype(jnp.float32)
            total += x * x
    return total


def tiled(count, body):
    def tile(i, carry):
        body(pl.ds(pl.multiple_of(i * 64, 64), 64))
        return carry

    lax.fori_loop(0, count // 64, tile, 0)


def wide_inverse(total):
    inv = lax.rsqrt(jnp.sum(total, axis=1, keepdims=True) / D + EPS)
    return jnp.broadcast_to(inv, total.shape)


def first_part_kernel(own, received, w, total_out, kv_out):
    refs = (own, received)

    def body(rows):
        total_out[rows, :] = row_squares(refs, rows)

    tiled(own.shape[1], body)
    kv_out[...] = product(blocks_of(refs), (w.at[:9],))


def first_kernel(other, w, total, kv_part, kv_out, inv_out):
    def body(rows):
        inv_out[rows, :] = wide_inverse(total[rows, :] + row_squares((other,), rows))

    tiled(other.shape[1], body)
    inv = inv_out[...]
    kv = kv_part[...] + product(blocks_of((other,)), (w.at[9:],))
    kv_out[...] = (kv * jnp.concatenate([inv, inv], axis=1)).astype(jnp.bfloat16)


def squares_kernel(own, received, total_out):
    def body(rows):
        total_out[rows, :] = row_squares((own, received), rows)

    tiled(own.shape[1], body)


def next_kernel(
    place, own, received, other, b_own, b_received, b_other, b_total, gain, w,
    kv_out, inv_out, stream, carried,
):
    ids = block_ids(place)
    mine = place[0] % 2
    refs = (own, received, other)
    b_refs = (b_own, b_received, b_other)

    def body(rows):
        def load(group, k):
            ref, j = part(group, k)
            return ref[j, rows, :].astype(jnp.float32)

        inv_post = wide_inverse(b_total[rows, :] + row_squares((b_other,), rows))
        total = jnp.zeros((64, BLK), jnp.float32)
        for k in range(NB):
            x = load(refs, k) + load(b_refs, k) * inv_post * gain_row(gain, 0, 1, ids[k])
            x = x.astype(jnp.bfloat16)
            stream[k, rows, :] = x
            x = x.astype(jnp.float32)
            total += x * x
        inv_out[rows, :] = wide_inverse(total)
        carried[rows, :] = stream[mine, rows, :]

    tiled(own.shape[1], body)
    inv = inv_out[...]
    kv = product(blocks_of((stream,)), (w,))
    kv_out[...] = (kv * jnp.concatenate([inv, inv], axis=1)).astype(jnp.bfloat16)


def grids():
    lane = lax.broadcasted_iota(jnp.int32, (BLK, BLK), 1)
    row = lax.broadcasted_iota(jnp.int32, (BLK, BLK), 0)
    return lane, row


def split_bias(bias, layer, h):
    low = bias[layer, h : h + 1, 0:BLK]
    high = bias[layer, h : h + 1, BLK : 2 * BLK]
    last = bias[layer, h : h + 1, 2 * BLK : 2 * BLK + 1]
    return low, high, last


def skewed(left, right):
    full = jnp.broadcast_to(jnp.concatenate([left, right], axis=1), (BLK, 2 * BLK))
    return pltpu.roll(full, 0, 1, stride=1, stride_axis=0)[:, :BLK].T


def padded_values(kv):
    values = kv[:, BLK:]
    lane = lax.broadcasted_iota(jnp.int32, values.shape, 1)
    one = jnp.ones_like(values)
    return jnp.where(lane < HEAD, values, one), jnp.where(lane < HEAD, one, values)


def head_scores(qh, keys):
    dims = (((1,), (1,)), ((), ()))
    return lax.dot_general(qh, keys, dims, preferred_element_type=jnp.float32)


def local_kernel(layer, x_count, *refs):
    xs, rest = refs[:x_count], refs[x_count:]
    w, inv, kv, bias, q_out, acc_out, top_out, sum_out, near_out = rest
    q = product(blocks_of(xs), (w,))
    q_out[...] = (q * inv[...] * HEAD ** (-0.5)).astype(jnp.bfloat16)
    lane, row = grids()
    values = padded_values(kv)
    tables = []
    for h in range(2):
        low, high, last = split_bias(bias, layer, h)
        last_row = jnp.broadcast_to(last, (1, BLK))
        diag = jnp.where((lane >= 64) & (row < 64), NEG, skewed(high, low))
        near_out[h] = skewed(last_row, high)
        tables.append((diag, near_out[h], jnp.broadcast_to(last, (BLK, BLK))))
    for i in range(4):
        rows = slice(i * BLK, (i + 1) * BLK)
        found = []
        for h in range(2):
            qh = q_out[rows, :]
            qh = jnp.where((lane < HEAD) == (h == 0), qh, jnp.zeros_like(qh))
            raw = head_scores(qh, kv[: (i + 1) * BLK, :BLK])
            scores = [
                raw[:, j * BLK : (j + 1) * BLK] + tables[h][min(i - j, 2)] for j in range(i + 1)
            ]
            top = jnp.max(functools.reduce(jnp.maximum, scores), axis=1, keepdims=True)
            weights = [jnp.exp(s - top).astype(jnp.bfloat16) for s in scores]
            probs = jnp.concatenate(weights, axis=1)
            acc = jnp.dot(probs, values[h][: (i + 1) * BLK], preferred_element_type=jnp.float32)
            found.append((acc, top))
        for n, out in enumerate((acc_out, top_out)):
            out[rows, :] = jnp.where(lane < HEAD, found[0][n], found[1][n])
        sum_out[rows, :] = jnp.where(lane < HEAD, found[1][0], found[0][0])


def merge_kernel(layer, first, q, kv, acc, top, total, nears, bias, out):
    lane, row = grids()
    values = padded_values(kv)
    hidden = jnp.where(first[0] == 1, NEG, 0.0)
    tables = []
    for h in range(2):
        last = split_bias(bias, layer, h)[2]
        full = jnp.broadcast_to(last, (BLK, BLK)) + hidden
        edge = jnp.where((lane < 64) & (row >= 64), NEG, full)
        tables.append((nears[h] + hidden, full, edge))
    where = [(i, h) for i in range(4) for h in range(2)]
    raw, peaks, olds, found = {}, {}, {}, {}
    for i, h in where:
        qh = q[i * BLK : (i + 1) * BLK, :]
        qh = jnp.where((lane < HEAD) == (h == 0), qh, jnp.zeros_like(qh))
        raw[i, h] = head_scores(qh, kv[i * BLK :, :BLK])
    for i, h in where:
        near, full, edge = tables[h]
        scores = []
        for j in range(4 - i):
            term = edge if j == 0 else near if j == 3 else full
            scores.append(raw[i, h][:, j * BLK : (j + 1) * BLK] + term)
        raw[i, h] = scores
        olds[i, h] = top[i * BLK : (i + 1) * BLK, h * HEAD : h * HEAD + 1]
        peak = jnp.max(functools.reduce(jnp.maximum, scores), axis=1, keepdims=True)
        peaks[i, h] = jnp.maximum(peak, olds[i, h])
    for i, h in where:
        weights = [jnp.exp(s - peaks[i, h]).astype(jnp.bfloat16) for s in raw[i, h]]
        probs = jnp.concatenate(weights, axis=1)
        found[i, h] = jnp.dot(probs, values[h][i * BLK :], preferred_element_type=jnp.float32)
    for i in range(4):
        rows = slice(i * BLK, (i + 1) * BLK)
        fades = [jnp.exp(olds[i, h] - peaks[i, h]) for h in range(2)]
        more, fade = (jnp.where(lane < HEAD, x, z) for x, z in ((found[i, 0], found[i, 1]), fades))
        sums = jnp.where(lane < HEAD, found[i, 1], found[i, 0])
        sums_fade = jnp.where(lane < HEAD, fades[1], fades[0])
        norm = pltpu.roll(total[rows, :] * sums_fade + sums, HEAD, 1)
        out[rows, :] = ((acc[rows, :] * fade + more) / norm).astype(jnp.bfloat16)


def rows_product(ids, offset, refs, w):
    rows = [
        w[pl.ds(pl.multiple_of(ids[offset + k] * BLK, BLK), BLK), :]
        for k in range(sum(ref.shape[0] for ref in refs))
    ]
    left = jnp.concatenate(blocks_of(refs), axis=1)
    return jnp.dot(left, jnp.concatenate(rows, axis=0), preferred_element_type=jnp.float32)


def out_part_kernel(place, own, received, w, acc):
    acc[...] = rows_product(block_ids(place), 0, (own, received), w)


def out_kernel(place, other, w, acc, out):
    out[...] = (acc[...] + rows_product(block_ids(place), 9, (other,), w)).astype(jnp.bfloat16)


def last_kernel(place, own, received, other, w, out, squares):
    out[...] = rows_product(block_ids(place), 0, (own, received, other), w)
    for i in range(4):
        x = out[i * BLK : (i + 1) * BLK, :]
        sums = jnp.sum((x * x).T, axis=0, keepdims=True)
        for n in range(NB):
            squares[n, i : i + 1, :] = sums


def finish_kernel(squares, branch, stream, gain, out):
    total = jnp.sum(squares[...], axis=0)
    inv = lax.rsqrt(total / D + EPS)
    for i in range(4):
        rows = slice(i * BLK, (i + 1) * BLK)
        scale = jnp.broadcast_to(inv[i : i + 1, :], (BLK, BLK)).T
        x = stream[rows, :].astype(jnp.float32)
        out[rows, :] = (x + branch[rows, :] * scale * gain[...]).astype(jnp.bfloat16)


def call(kernel, ins, outs, scratch, mib, flops, args):
    size = sum(a.size * a.dtype.itemsize for a in args)
    return pl.pallas_call(
        kernel,
        out_shape=outs,
        in_specs=ins,
        out_specs=jax.tree.map(lambda _: VMEM, outs),
        scratch_shapes=scratch,
        compiler_params=params(mib),
        cost_estimate=pl.CostEstimate(flops=flops, bytes_accessed=size, transcendentals=0),
    )(*args)


def on_device(residual, gains, w_query, w_key, w_value, w_out, rel_bias):
    tokens = residual.shape[0]
    half = jnp.bfloat16
    place = lax.axis_index(("y", "c")).reshape(1).astype(jnp.int32)
    first = (lax.axis_index("sp") == 0).reshape(1).astype(jnp.int32)
    block = jax.ShapeDtypeStruct((tokens, BLK), half)
    pair = jax.ShapeDtypeStruct((tokens, 2 * BLK), half)
    wide = jax.ShapeDtypeStruct((tokens, BLK), jnp.float32)
    stack = jax.ShapeDtypeStruct((NB, tokens, BLK), half)
    tiles = jax.ShapeDtypeStruct((2, BLK, BLK), jnp.float32)
    flow = lax.axis_size("sp")
    shift = [(i, i + 1) for i in range(flow - 1)]

    def scaled(layer, weights, mib):
        count = len(weights)
        shape = jax.ShapeDtypeStruct((NB, BLK, count * BLK), half)
        scratch = [pltpu.VMEM((D, BLK), half)] * count + [pltpu.SemaphoreType.DMA((count, CUTS))]
        return call(
            functools.partial(scale_kernel, layer, count), [SMEM, VMEM] + [HBM] * count,
            shape, scratch, mib, 10**9, (place, gains, *weights),
        )

    def attention(layer, xs, wq, kv, inv):
        previous = lax.ppermute(kv, "sp", shift)
        local = call(
            functools.partial(local_kernel, layer, len(xs)), [VMEM] * (len(xs) + 4),
            (block, wide, wide, wide, tiles), [], 4, 2 * 10**9, (*xs, wq, inv, kv, rel_bias),
        )
        return call(
            functools.partial(merge_kernel, layer), [SMEM] + [VMEM] * 7, block, [], 4,
            10**9, (first, local[0], previous, *local[1:], rel_bias),
        )

    def projected(attended, w):
        own, received, other = attended
        acc = call(
            out_part_kernel, [SMEM] + [VMEM] * 3, wide, [], 4, 10**9, (place, own, received, w)
        )
        return other, w, acc

    wkv = scaled(0, (w_key, w_value), BIG)
    wq = scaled(0, (w_query,), 4)
    stream = gather_blocks(residual)
    parts = call(
        first_part_kernel, [VMEM] * 3,
        (wide, jax.ShapeDtypeStruct((tokens, 2 * BLK), jnp.float32)), [], 4, 10**9,
        (*stream[:2], wkv),
    )
    kv, inv = call(
        first_kernel, [VMEM] * 4, (pair, wide), [], 4, 10**9, (stream[2], wkv, *parts),
    )
    attended = gather_blocks(attention(0, stream, wq, kv, inv))
    branch = call(
        out_kernel, [SMEM] + [VMEM] * 3, block, [], 4, 10**9,
        (place, *projected(attended, w_out[0])),
    )
    branch = gather_blocks(branch)
    total = call(squares_kernel, [VMEM] * 2, wide, [], 4, 10**9, branch[:2])
    wkv = scaled(1, (w_key, w_value), 4)
    wq = scaled(1, (w_query,), 4)
    kv, inv, full, carried = call(
        next_kernel, [SMEM] + [VMEM] * 9, (pair, wide, stack, block), [], 4, 2 * 10**9,
        (place, *stream, *branch, total, gains, wkv),
    )
    attended = gather_blocks(attention(1, (full,), wq, kv, inv))
    branch, squares = call(
        last_kernel, [SMEM] + [VMEM] * 4,
        (wide, jax.ShapeDtypeStruct((NB, tokens // BLK, BLK), jnp.float32)), [], 4, 10**9,
        (place, *attended, w_out[1]),
    )
    own_gain = lax.dynamic_slice_in_dim(
        gains[1, 1].reshape(1, D), lax.axis_index(("y", "c")) * BLK, BLK, 1
    )
    everything = lax.all_to_all(squares, ("y", "c"), split_axis=0, concat_axis=0, tiled=True)
    return call(
        finish_kernel, [VMEM] * 4, block, [], 4, 10**7, (everything, branch, carried, own_gain)
    )


def solution(mesh):
    finer = Mesh(mesh.devices.reshape(mesh.shape["sp"], 8, 2), ("sp", "y", "c"))
    tp = ("y", "c")
    in_specs = (
        P("sp", tp),
        P(),
        P(None, None, tp),
        P(None, None, tp),
        P(None, None, tp),
        P(None, None, tp),
        P(None, tp, None),
    )

    return jax.shard_map(
        on_device, mesh=finer, in_specs=in_specs, out_specs=P("sp", tp), check_vma=False
    )
```

```python
import functools

import jax
import jax.numpy as jnp
from jax import lax
from jax.experimental import pallas as pl
from jax.experimental.pallas import tpu as pltpu
from jax.sharding import Mesh
from jax.sharding import PartitionSpec as P


D = 2048
HEAD = 64
BLK = 128
NB = 16
EPS = 1e-06
BIG = 60
CUTS = 4
NEG = -1e30
VMEM = pl.BlockSpec(memory_space=pltpu.VMEM)
SMEM = pl.BlockSpec(memory_space=pltpu.SMEM)
HBM = pl.BlockSpec(memory_space=pltpu.HBM)


def params(mib):
    return pltpu.CompilerParams(vmem_limit_bytes=mib * 1024 * 1024)


def core_pairs(step):
    pairs = []
    for y in range(8):
        for c in range(2):
            target = (y + (step if c == 0 else -step)) % 8
            pairs.append((2 * y + c, 2 * target + c))
    return pairs


def gather_blocks(x, own=None):
    core = lax.axis_index("c")

    if own is None:
        own = lax.all_gather(x, "c", axis=0)
    two = lax.ppermute(own, ("y", "c"), core_pairs(2))
    one = lax.ppermute(own, ("y", "c"), core_pairs(1))
    half = lax.dynamic_index_in_dim(two, core, 0, keepdims=True)
    three = lax.ppermute(two, ("y", "c"), core_pairs(1))
    four = lax.ppermute(half, ("y", "c"), core_pairs(2))
    received = jnp.concatenate([one, two, three, four], axis=0)
    other = lax.ppermute(received, "c", [(0, 1), (1, 0)])
    return own, received, other


def block_ids(place):
    y, c = place[0] // 2, place[0] % 2
    sign = 1 - 2 * c
    across = 2 * ((y + 4) % 8)
    ids = [2 * y, 2 * y + 1]
    for way, last in ((-sign, c), (sign, 1 - c)):
        for d in (1, 2, 3):
            chip = (y + way * d + 8) % 8
            ids += [2 * chip, 2 * chip + 1]
        ids.append(across + last)
    return ids


def part(refs, k):
    own, received, other = refs
    if k < 2:
        return own, k
    if k < 9:
        return received, k - 2
    return other, k - 9


def scale_kernel(layer, count, place, gain, *refs):
    weights, (out, *held, sems) = refs[:count], refs[count:]
    ids = block_ids(place)
    copies = []
    for n, (w, dst) in enumerate(zip(weights, held)):
        for m in range(CUTS):
            rows = pl.ds(m * (D // CUTS), D // CUTS)
            copies.append(
                pltpu.make_async_copy(w.at[layer, rows, :], dst.at[rows, :], sems.at[n, m])
            )
    for copy in copies:
        copy.start()
    for copy in copies:
        copy.wait()
    for k in range(NB):
        t = ids[k]
        rows = pl.ds(pl.multiple_of(t * BLK, BLK), BLK)
        factor = jnp.broadcast_to(gain_row(gain, layer, 0, t), (BLK, BLK)).T
        for n, w in enumerate(held):
            scaled = w[rows, :].astype(jnp.float32) * factor
            out[k, :, n * BLK : (n + 1) * BLK] = scaled.astype(jnp.bfloat16)


def gain_row(gain, layer, kind, t):
    return gain[layer, kind : kind + 1, pl.ds(pl.multiple_of(t * BLK, BLK), BLK)]


def product(blocks, weights):
    left = jnp.concatenate(blocks, axis=1)
    right = jnp.concatenate(
        [jnp.concatenate([w[k] for w in weights], axis=1) for k in range(len(blocks))], axis=0
    )
    return jnp.dot(left, right, preferred_element_type=jnp.float32)


def blocks_of(refs):
    return [ref[k] for ref in refs for k in range(ref.shape[0])]


def row_squares(refs, rows):
    total = jnp.zeros((rows.size, BLK), jnp.float32)
    for ref in refs:
        for k in range(ref.shape[0]):
            x = ref[k, rows, :].astype(jnp.float32)
            total += x * x
    return total


def tiled(count, body):
    def tile(i, carry):
        body(pl.ds(pl.multiple_of(i * 64, 64), 64))
        return carry

    lax.fori_loop(0, count // 64, tile, 0)


def wide_inverse(total):
    inv = lax.rsqrt(jnp.sum(total, axis=1, keepdims=True) / D + EPS)
    return jnp.broadcast_to(inv, total.shape)


def first_part_kernel(own, received, w, total_out, kv_out):
    refs = (own, received)

    def body(rows):
        total_out[rows, :] = row_squares(refs, rows)

    tiled(own.shape[1], body)
    kv_out[...] = product(blocks_of(refs), (w.at[:9],))


def first_kernel(other, w, total, kv_part, kv_out, inv_out):
    def body(rows):
        inv_out[rows, :] = wide_inverse(total[rows, :] + row_squares((other,), rows))

    tiled(other.shape[1], body)
    inv = inv_out[...]
    kv = kv_part[...] + product(blocks_of((other,)), (w.at[9:],))
    kv_out[...] = (kv * jnp.concatenate([inv, inv], axis=1)).astype(jnp.bfloat16)


def squares_kernel(own, received, total_out):
    def body(rows):
        total_out[rows, :] = row_squares((own, received), rows)

    tiled(own.shape[1], body)


def next_kernel(
    place, own, received, other, b_own, b_received, b_other, b_total, gain, w,
    kv_out, inv_out, stream, carried,
):
    ids = block_ids(place)
    mine = place[0] % 2
    refs = (own, received, other)
    b_refs = (b_own, b_received, b_other)

    def body(rows):
        def load(group, k):
            ref, j = part(group, k)
            return ref[j, rows, :].astype(jnp.float32)

        inv_post = wide_inverse(b_total[rows, :] + row_squares((b_other,), rows))
        total = jnp.zeros((64, BLK), jnp.float32)
        for k in range(NB):
            x = load(refs, k) + load(b_refs, k) * inv_post * gain_row(gain, 0, 1, ids[k])
            x = x.astype(jnp.bfloat16)
            stream[k, rows, :] = x
            x = x.astype(jnp.float32)
            total += x * x
        inv_out[rows, :] = wide_inverse(total)
        carried[rows, :] = stream[mine, rows, :]

    tiled(own.shape[1], body)
    inv = inv_out[...]
    kv = product(blocks_of((stream,)), (w,))
    kv_out[...] = (kv * jnp.concatenate([inv, inv], axis=1)).astype(jnp.bfloat16)


def grids():
    lane = lax.broadcasted_iota(jnp.int32, (BLK, BLK), 1)
    row = lax.broadcasted_iota(jnp.int32, (BLK, BLK), 0)
    return lane, row


def split_bias(bias, layer, h):
    low = bias[layer, h : h + 1, 0:BLK]
    high = bias[layer, h : h + 1, BLK : 2 * BLK]
    last = bias[layer, h : h + 1, 2 * BLK : 2 * BLK + 1]
    return low, high, last


def skewed(left, right):
    full = jnp.broadcast_to(jnp.concatenate([left, right], axis=1), (BLK, 2 * BLK))
    return pltpu.roll(full, 0, 1, stride=1, stride_axis=0)[:, :BLK].T


def padded_values(kv):
    values = kv[:, BLK:]
    lane = lax.broadcasted_iota(jnp.int32, values.shape, 1)
    one = jnp.ones_like(values)
    return jnp.where(lane < HEAD, values, one), jnp.where(lane < HEAD, one, values)


def head_scores(qh, keys):
    dims = (((1,), (1,)), ((), ()))
    return lax.dot_general(qh, keys, dims, preferred_element_type=jnp.float32)


def local_kernel(layer, x_count, *refs):
    xs, rest = refs[:x_count], refs[x_count:]
    w, inv, kv, bias, q_out, acc_out, top_out, sum_out, near_out = rest
    q = product(blocks_of(xs), (w,))
    q_out[...] = (q * inv[...] * HEAD ** (-0.5)).astype(jnp.bfloat16)
    lane, row = grids()
    values = padded_values(kv)
    tables = []
    for h in range(2):
        low, high, last = split_bias(bias, layer, h)
        last_row = jnp.broadcast_to(last, (1, BLK))
        diag = jnp.where((lane >= 64) & (row < 64), NEG, skewed(high, low))
        near_out[h] = skewed(last_row, high)
        tables.append((diag, near_out[h], jnp.broadcast_to(last, (BLK, BLK))))
    for i in range(4):
        rows = slice(i * BLK, (i + 1) * BLK)
        found = []
        for h in range(2):
            qh = q_out[rows, :]
            qh = jnp.where((lane < HEAD) == (h == 0), qh, jnp.zeros_like(qh))
            raw = head_scores(qh, kv[: (i + 1) * BLK, :BLK])
            scores = [
                raw[:, j * BLK : (j + 1) * BLK] + tables[h][min(i - j, 2)] for j in range(i + 1)
            ]
            top = jnp.max(functools.reduce(jnp.maximum, scores), axis=1, keepdims=True)
            weights = [jnp.exp(s - top).astype(jnp.bfloat16) for s in scores]
            probs = jnp.concatenate(weights, axis=1)
            acc = jnp.dot(probs, values[h][: (i + 1) * BLK], preferred_element_type=jnp.float32)
            found.append((acc, top))
        for n, out in enumerate((acc_out, top_out)):
            out[rows, :] = jnp.where(lane < HEAD, found[0][n], found[1][n])
        sum_out[rows, :] = jnp.where(lane < HEAD, found[1][0], found[0][0])


def merge_kernel(layer, first, q, kv, acc, top, total, nears, bias, out):
    lane, row = grids()
    values = padded_values(kv)
    hidden = jnp.where(first[0] == 1, NEG, 0.0)
    tables = []
    for h in range(2):
        last = split_bias(bias, layer, h)[2]
        full = jnp.broadcast_to(last, (BLK, BLK)) + hidden
        edge = jnp.where((lane < 64) & (row >= 64), NEG, full)
        tables.append((nears[h] + hidden, full, edge))
    where = [(i, h) for i in range(4) for h in range(2)]
    raw, peaks, olds, found = {}, {}, {}, {}
    for i, h in where:
        qh = q[i * BLK : (i + 1) * BLK, :]
        qh = jnp.where((lane < HEAD) == (h == 0), qh, jnp.zeros_like(qh))
        raw[i, h] = head_scores(qh, kv[i * BLK :, :BLK])
    for i, h in where:
        near, full, edge = tables[h]
        scores = []
        for j in range(4 - i):
            term = edge if j == 0 else near if j == 3 else full
            scores.append(raw[i, h][:, j * BLK : (j + 1) * BLK] + term)
        raw[i, h] = scores
        olds[i, h] = top[i * BLK : (i + 1) * BLK, h * HEAD : h * HEAD + 1]
        peak = jnp.max(functools.reduce(jnp.maximum, scores), axis=1, keepdims=True)
        peaks[i, h] = jnp.maximum(peak, olds[i, h])
    for i, h in where:
        weights = [jnp.exp(s - peaks[i, h]).astype(jnp.bfloat16) for s in raw[i, h]]
        probs = jnp.concatenate(weights, axis=1)
        found[i, h] = jnp.dot(probs, values[h][i * BLK :], preferred_element_type=jnp.float32)
    for i in range(4):
        rows = slice(i * BLK, (i + 1) * BLK)
        fades = [jnp.exp(olds[i, h] - peaks[i, h]) for h in range(2)]
        more, fade = (jnp.where(lane < HEAD, x, z) for x, z in ((found[i, 0], found[i, 1]), fades))
        sums = jnp.where(lane < HEAD, found[i, 1], found[i, 0])
        sums_fade = jnp.where(lane < HEAD, fades[1], fades[0])
        norm = pltpu.roll(total[rows, :] * sums_fade + sums, HEAD, 1)
        out[rows, :] = ((acc[rows, :] * fade + more) / norm).astype(jnp.bfloat16)


def rows_product(layer, ids, offset, refs, weights):
    count = sum(ref.shape[0] for ref in refs)
    rows = [
        pl.ds(pl.multiple_of(ids[offset + k] * BLK, BLK), BLK) for k in range(count)
    ]
    right = jnp.concatenate(
        [jnp.concatenate([w[layer, r, :] for w in weights], axis=1) for r in rows], axis=0
    )
    left = jnp.concatenate(blocks_of(refs), axis=1)
    return jnp.dot(left, right, preferred_element_type=jnp.float32)


def out_part_kernel(place, own, received, w, w_other, acc):
    acc[...] = rows_product(0, block_ids(place), 0, (own, received), (w, w_other))


def out_kernel(place, other, w, w_other, acc, out):
    core = place[0] % 2
    total = acc[...] + rows_product(0, block_ids(place), 9, (other,), (w, w_other))
    out[core] = total[:, :BLK].astype(jnp.bfloat16)
    out[1 - core] = total[:, BLK:].astype(jnp.bfloat16)


def last_kernel(place, own, received, other, w, out, squares):
    out[...] = rows_product(1, block_ids(place), 0, (own, received, other), (w,))
    for i in range(4):
        x = out[i * BLK : (i + 1) * BLK, :]
        sums = jnp.sum((x * x).T, axis=0, keepdims=True)
        for n in range(NB):
            squares[n, i : i + 1, :] = sums


def finish_kernel(squares, branch, stream, gain, out):
    total = jnp.sum(squares[...], axis=0)
    inv = lax.rsqrt(total / D + EPS)
    for i in range(4):
        rows = slice(i * BLK, (i + 1) * BLK)
        scale = jnp.broadcast_to(inv[i : i + 1, :], (BLK, BLK)).T
        x = stream[rows, :].astype(jnp.float32)
        out[rows, :] = (x + branch[rows, :] * scale * gain[...]).astype(jnp.bfloat16)


def call(kernel, ins, outs, scratch, mib, flops, args):
    size = sum(a.size * a.dtype.itemsize for a in args)
    return pl.pallas_call(
        kernel,
        out_shape=outs,
        in_specs=ins,
        out_specs=jax.tree.map(lambda _: VMEM, outs),
        scratch_shapes=scratch,
        compiler_params=params(mib),
        cost_estimate=pl.CostEstimate(flops=flops, bytes_accessed=size, transcendentals=0),
    )(*args)


def on_device(residual, gains, w_query, w_key, w_value, w_out, rel_bias):
    tokens = residual.shape[0]
    half = jnp.bfloat16
    place = lax.axis_index(("y", "c")).reshape(1).astype(jnp.int32)
    first = (lax.axis_index("sp") == 0).reshape(1).astype(jnp.int32)
    block = jax.ShapeDtypeStruct((tokens, BLK), half)
    pair = jax.ShapeDtypeStruct((tokens, 2 * BLK), half)
    wide = jax.ShapeDtypeStruct((tokens, BLK), jnp.float32)
    stack = jax.ShapeDtypeStruct((NB, tokens, BLK), half)
    tiles = jax.ShapeDtypeStruct((2, BLK, BLK), jnp.float32)
    flow = lax.axis_size("sp")
    shift = [(i, i + 1) for i in range(flow - 1)]

    def scaled(layer, weights, mib):
        count = len(weights)
        shape = jax.ShapeDtypeStruct((NB, BLK, count * BLK), half)
        scratch = [pltpu.VMEM((D, BLK), half)] * count + [pltpu.SemaphoreType.DMA((count, CUTS))]
        return call(
            functools.partial(scale_kernel, layer, count), [SMEM, VMEM] + [HBM] * count,
            shape, scratch, mib, 10**9, (place, gains, *weights),
        )

    def attention(layer, xs, wq, kv, inv):
        previous = lax.ppermute(kv, "sp", shift)
        local = call(
            functools.partial(local_kernel, layer, len(xs)), [VMEM] * (len(xs) + 4),
            (block, wide, wide, wide, tiles), [], 4, 2 * 10**9, (*xs, wq, inv, kv, rel_bias),
        )
        return call(
            functools.partial(merge_kernel, layer), [SMEM] + [VMEM] * 7, block, [], 4,
            10**9, (first, local[0], previous, *local[1:], rel_bias),
        )

    w_other = lax.ppermute(w_out, "c", [(0, 1), (1, 0)])
    both = jax.ShapeDtypeStruct((2, tokens, BLK), half)
    double = jax.ShapeDtypeStruct((tokens, 2 * BLK), jnp.float32)
    wkv = scaled(0, (w_key, w_value), BIG)
    wq = scaled(0, (w_query,), 4)
    stream = gather_blocks(residual)
    parts = call(
        first_part_kernel, [VMEM] * 3,
        (wide, jax.ShapeDtypeStruct((tokens, 2 * BLK), jnp.float32)), [], 4, 10**9,
        (*stream[:2], wkv),
    )
    kv, inv = call(
        first_kernel, [VMEM] * 4, (pair, wide), [], 4, 10**9, (stream[2], wkv, *parts),
    )
    attended = gather_blocks(attention(0, stream, wq, kv, inv))
    acc = call(
        out_part_kernel, [SMEM] + [VMEM] * 4, double, [], 4, 10**9,
        (place, *attended[:2], w_out, w_other),
    )
    branch = call(
        out_kernel, [SMEM] + [VMEM] * 4, both, [], 4, 10**9,
        (place, attended[2], w_out, w_other, acc),
    )
    branch = gather_blocks(None, branch)
    total = call(squares_kernel, [VMEM] * 2, wide, [], 4, 10**9, branch[:2])
    wkv = scaled(1, (w_key, w_value), 4)
    wq = scaled(1, (w_query,), 4)
    kv, inv, full, carried = call(
        next_kernel, [SMEM] + [VMEM] * 9, (pair, wide, stack, block), [], 4, 2 * 10**9,
        (place, *stream, *branch, total, gains, wkv),
    )
    attended = gather_blocks(attention(1, (full,), wq, kv, inv))
    branch, squares = call(
        last_kernel, [SMEM] + [VMEM] * 4,
        (wide, jax.ShapeDtypeStruct((NB, tokens // BLK, BLK), jnp.float32)), [], 4, 10**9,
        (place, *attended, w_out),
    )
    own_gain = lax.dynamic_slice_in_dim(
        gains[1, 1].reshape(1, D), lax.axis_index(("y", "c")) * BLK, BLK, 1
    )
    everything = lax.all_to_all(squares, ("y", "c"), split_axis=0, concat_axis=0, tiled=True)
    return call(
        finish_kernel, [VMEM] * 4, block, [], 4, 10**7, (everything, branch, carried, own_gain)
    )


def solution(mesh):
    finer = Mesh(mesh.devices.reshape(mesh.shape["sp"], 8, 2), ("sp", "y", "c"))
    tp = ("y", "c")
    in_specs = (
        P("sp", tp),
        P(),
        P(None, None, tp),
        P(None, None, tp),
        P(None, None, tp),
        P(None, None, tp),
        P(None, tp, None),
    )

    return jax.shard_map(
        on_device, mesh=finer, in_specs=in_specs, out_specs=P("sp", tp), check_vma=False
    )
```

```python
import functools

import jax
import jax.numpy as jnp
from jax import lax
from jax.experimental import pallas as pl
from jax.experimental.pallas import tpu as pltpu
from jax.sharding import Mesh
from jax.sharding import PartitionSpec as P


D = 2048
HEAD = 64
BLK = 128
NB = 16
EPS = 1e-06
BIG = 60
CUTS = 8
TILE = 128
NEG = -1e30
VMEM = pl.BlockSpec(memory_space=pltpu.VMEM)
SMEM = pl.BlockSpec(memory_space=pltpu.SMEM)
HBM = pl.BlockSpec(memory_space=pltpu.HBM)


def params(mib):
    return pltpu.CompilerParams(vmem_limit_bytes=mib * 1024 * 1024)


def core_pairs(step):
    pairs = []
    for y in range(8):
        for c in range(2):
            target = (y + (step if c == 0 else -step)) % 8
            pairs.append((2 * y + c, 2 * target + c))
    return pairs


def gather_blocks(x, own=None):
    core = lax.axis_index("c")

    if own is None:
        own = lax.all_gather(x, "c", axis=0)
    two = lax.ppermute(own, ("y", "c"), core_pairs(2))
    one = lax.ppermute(own, ("y", "c"), core_pairs(1))
    half = lax.dynamic_index_in_dim(two, core, 0, keepdims=True)
    three = lax.ppermute(two, ("y", "c"), core_pairs(1))
    four = lax.ppermute(half, ("y", "c"), core_pairs(2))
    received = jnp.concatenate([one, two, three, four], axis=0)
    other = lax.ppermute(received, "c", [(0, 1), (1, 0)])
    return own, received, other


def block_ids(place):
    y, c = place[0] // 2, place[0] % 2
    sign = 1 - 2 * c
    across = 2 * ((y + 4) % 8)
    ids = [2 * y, 2 * y + 1]
    for way, last in ((-sign, c), (sign, 1 - c)):
        for d in (1, 2, 3):
            chip = (y + way * d + 8) % 8
            ids += [2 * chip, 2 * chip + 1]
        ids.append(across + last)
    return ids


def part(refs, k):
    own, received, other = refs
    if k < 2:
        return own, k
    if k < 9:
        return received, k - 2
    return other, k - 9


def scale_kernel(layer, count, place, gain, *refs):
    weights, (out, *held, sems) = refs[:count], refs[count:]
    ids = block_ids(place)
    copies = []
    for n, (w, dst) in enumerate(zip(weights, held)):
        for m in range(CUTS):
            rows = pl.ds(m * (D // CUTS), D // CUTS)
            copies.append(
                pltpu.make_async_copy(w.at[layer, rows, :], dst.at[rows, :], sems.at[n, m])
            )
    for copy in copies:
        copy.start()
    for copy in copies:
        copy.wait()
    for k in range(NB):
        t = ids[k]
        rows = pl.ds(pl.multiple_of(t * BLK, BLK), BLK)
        factor = jnp.broadcast_to(gain_row(gain, layer, 0, t), (BLK, BLK)).T
        for n, w in enumerate(held):
            scaled = w[rows, :].astype(jnp.float32) * factor
            out[k, :, n * BLK : (n + 1) * BLK] = scaled.astype(jnp.bfloat16)


def gain_row(gain, layer, kind, t):
    return gain[layer, kind : kind + 1, pl.ds(pl.multiple_of(t * BLK, BLK), BLK)]


def product(blocks, weights):
    left = jnp.concatenate(blocks, axis=1)
    right = jnp.concatenate(
        [jnp.concatenate([w[k] for w in weights], axis=1) for k in range(len(blocks))], axis=0
    )
    return jnp.dot(left, right, preferred_element_type=jnp.float32)


def blocks_of(refs):
    return [ref[k] for ref in refs for k in range(ref.shape[0])]


def row_squares(refs, rows):
    total = jnp.zeros((rows.size, BLK), jnp.float32)
    for ref in refs:
        for k in range(ref.shape[0]):
            x = ref[k, rows, :].astype(jnp.float32)
            total += x * x
    return total


def tiled(count, body):
    for i in range(count // TILE):
        body(pl.ds(i * TILE, TILE))


def wide_inverse(total):
    inv = lax.rsqrt(jnp.sum(total, axis=1, keepdims=True) / D + EPS)
    return jnp.broadcast_to(inv, total.shape)


def first_part_kernel(own, received, w, total_out, kv_out):
    refs = (own, received)

    def body(rows):
        total_out[rows, :] = row_squares(refs, rows)

    tiled(own.shape[1], body)
    kv_out[...] = product(blocks_of(refs), (w.at[:9],))


def first_kernel(other, w, total, kv_part, kv_out, inv_out):
    def body(rows):
        inv_out[rows, :] = wide_inverse(total[rows, :] + row_squares((other,), rows))

    tiled(other.shape[1], body)
    inv = inv_out[...]
    kv = kv_part[...] + product(blocks_of((other,)), (w.at[9:],))
    kv_out[...] = (kv * jnp.concatenate([inv, inv], axis=1)).astype(jnp.bfloat16)


def squares_kernel(own, received, total_out):
    def body(rows):
        total_out[rows, :] = row_squares((own, received), rows)

    tiled(own.shape[1], body)


def next_kernel(
    place, own, received, other, b_own, b_received, b_other, b_total, gain, w,
    kv_out, inv_out, stream, carried,
):
    ids = block_ids(place)
    mine = place[0] % 2
    refs = (own, received, other)
    b_refs = (b_own, b_received, b_other)

    def body(rows):
        def load(group, k):
            ref, j = part(group, k)
            return ref[j, rows, :].astype(jnp.float32)

        inv_post = wide_inverse(b_total[rows, :] + row_squares((b_other,), rows))
        total = jnp.zeros((TILE, BLK), jnp.float32)
        for k in range(NB):
            x = load(refs, k) + load(b_refs, k) * inv_post * gain_row(gain, 0, 1, ids[k])
            x = x.astype(jnp.bfloat16)
            stream[k, rows, :] = x
            x = x.astype(jnp.float32)
            total += x * x
        inv_out[rows, :] = wide_inverse(total)
        carried[rows, :] = stream[mine, rows, :]

    tiled(own.shape[1], body)
    inv = inv_out[...]
    kv = product(blocks_of((stream,)), (w,))
    kv_out[...] = (kv * jnp.concatenate([inv, inv], axis=1)).astype(jnp.bfloat16)


def grids():
    lane = lax.broadcasted_iota(jnp.int32, (BLK, BLK), 1)
    row = lax.broadcasted_iota(jnp.int32, (BLK, BLK), 0)
    return lane, row


def split_bias(bias, layer, h):
    low = bias[layer, h : h + 1, 0:BLK]
    high = bias[layer, h : h + 1, BLK : 2 * BLK]
    last = bias[layer, h : h + 1, 2 * BLK : 2 * BLK + 1]
    return low, high, last


def skewed(left, right):
    full = jnp.broadcast_to(jnp.concatenate([left, right], axis=1), (BLK, 2 * BLK))
    return pltpu.roll(full, 0, 1, stride=1, stride_axis=0)[:, :BLK].T


def padded_values(kv):
    values = kv[:, BLK:]
    lane = lax.broadcasted_iota(jnp.int32, values.shape, 1)
    one = jnp.ones_like(values)
    return jnp.where(lane < HEAD, values, one), jnp.where(lane < HEAD, one, values)


def head_scores(qh, keys):
    dims = (((1,), (1,)), ((), ()))
    return lax.dot_general(qh, keys, dims, preferred_element_type=jnp.float32)


def local_kernel(layer, x_count, *refs):
    xs, rest = refs[:x_count], refs[x_count:]
    w, inv, kv, bias, q_out, acc_out, top_out, sum_out, near_out = rest
    q = product(blocks_of(xs), (w,))
    q_out[...] = (q * inv[...] * HEAD ** (-0.5)).astype(jnp.bfloat16)
    lane, row = grids()
    values = padded_values(kv)
    tables = []
    for h in range(2):
        low, high, last = split_bias(bias, layer, h)
        last_row = jnp.broadcast_to(last, (1, BLK))
        diag = jnp.where((lane >= 64) & (row < 64), NEG, skewed(high, low))
        near_out[h] = skewed(last_row, high)
        tables.append((diag, near_out[h], jnp.broadcast_to(last, (BLK, BLK))))
    for i in range(4):
        rows = slice(i * BLK, (i + 1) * BLK)
        found = []
        for h in range(2):
            qh = q_out[rows, :]
            qh = jnp.where((lane < HEAD) == (h == 0), qh, jnp.zeros_like(qh))
            raw = head_scores(qh, kv[: (i + 1) * BLK, :BLK])
            scores = [
                raw[:, j * BLK : (j + 1) * BLK] + tables[h][min(i - j, 2)] for j in range(i + 1)
            ]
            top = jnp.max(functools.reduce(jnp.maximum, scores), axis=1, keepdims=True)
            weights = [jnp.exp(s - top).astype(jnp.bfloat16) for s in scores]
            probs = jnp.concatenate(weights, axis=1)
            acc = jnp.dot(probs, values[h][: (i + 1) * BLK], preferred_element_type=jnp.float32)
            found.append((acc, top))
        for n, out in enumerate((acc_out, top_out)):
            out[rows, :] = jnp.where(lane < HEAD, found[0][n], found[1][n])
        sum_out[rows, :] = jnp.where(lane < HEAD, found[1][0], found[0][0])


def merge_kernel(layer, first, q, kv, acc, top, total, nears, bias, out):
    lane, row = grids()
    values = padded_values(kv)
    hidden = jnp.where(first[0] == 1, NEG, 0.0)
    tables = []
    for h in range(2):
        last = split_bias(bias, layer, h)[2]
        full = jnp.broadcast_to(last, (BLK, BLK)) + hidden
        edge = jnp.where((lane < 64) & (row >= 64), NEG, full)
        tables.append((nears[h] + hidden, full, edge))
    where = [(i, h) for i in range(4) for h in range(2)]
    raw, peaks, olds, found = {}, {}, {}, {}
    for i, h in where:
        qh = q[i * BLK : (i + 1) * BLK, :]
        qh = jnp.where((lane < HEAD) == (h == 0), qh, jnp.zeros_like(qh))
        raw[i, h] = head_scores(qh, kv[i * BLK :, :BLK])
    for i, h in where:
        near, full, edge = tables[h]
        scores = []
        for j in range(4 - i):
            term = edge if j == 0 else near if j == 3 else full
            scores.append(raw[i, h][:, j * BLK : (j + 1) * BLK] + term)
        raw[i, h] = scores
        olds[i, h] = top[i * BLK : (i + 1) * BLK, h * HEAD : h * HEAD + 1]
        peak = jnp.max(functools.reduce(jnp.maximum, scores), axis=1, keepdims=True)
        peaks[i, h] = jnp.maximum(peak, olds[i, h])
    for i, h in where:
        weights = [jnp.exp(s - peaks[i, h]).astype(jnp.bfloat16) for s in raw[i, h]]
        probs = jnp.concatenate(weights, axis=1)
        found[i, h] = jnp.dot(probs, values[h][i * BLK :], preferred_element_type=jnp.float32)
    for i in range(4):
        rows = slice(i * BLK, (i + 1) * BLK)
        fades = [jnp.exp(olds[i, h] - peaks[i, h]) for h in range(2)]
        more, fade = (jnp.where(lane < HEAD, x, z) for x, z in ((found[i, 0], found[i, 1]), fades))
        sums = jnp.where(lane < HEAD, found[i, 1], found[i, 0])
        sums_fade = jnp.where(lane < HEAD, fades[1], fades[0])
        norm = pltpu.roll(total[rows, :] * sums_fade + sums, HEAD, 1)
        out[rows, :] = ((acc[rows, :] * fade + more) / norm).astype(jnp.bfloat16)


def rows_product(layer, ids, offset, refs, weights):
    count = sum(ref.shape[0] for ref in refs)
    rows = [
        pl.ds(pl.multiple_of(ids[offset + k] * BLK, BLK), BLK) for k in range(count)
    ]
    right = jnp.concatenate(
        [jnp.concatenate([w[layer, r, :] for w in weights], axis=1) for r in rows], axis=0
    )
    left = jnp.concatenate(blocks_of(refs), axis=1)
    return jnp.dot(left, right, preferred_element_type=jnp.float32)


def out_part_kernel(place, own, received, w, w_other, acc):
    acc[...] = rows_product(0, block_ids(place), 0, (own, received), (w, w_other))


def out_kernel(place, other, w, w_other, acc, out):
    core = place[0] % 2
    total = acc[...] + rows_product(0, block_ids(place), 9, (other,), (w, w_other))
    out[core] = total[:, :BLK].astype(jnp.bfloat16)
    out[1 - core] = total[:, BLK:].astype(jnp.bfloat16)


def last_kernel(place, own, received, other, w, out, squares):
    out[...] = rows_product(1, block_ids(place), 0, (own, received, other), (w,))
    for i in range(4):
        x = out[i * BLK : (i + 1) * BLK, :]
        sums = jnp.sum((x * x).T, axis=0, keepdims=True)
        for n in range(NB):
            squares[n, i : i + 1, :] = sums


def finish_kernel(squares, branch, stream, gain, out):
    total = jnp.sum(squares[...], axis=0)
    inv = lax.rsqrt(total / D + EPS)
    for i in range(4):
        rows = slice(i * BLK, (i + 1) * BLK)
        scale = jnp.broadcast_to(inv[i : i + 1, :], (BLK, BLK)).T
        x = stream[rows, :].astype(jnp.float32)
        out[rows, :] = (x + branch[rows, :] * scale * gain[...]).astype(jnp.bfloat16)


def call(kernel, ins, outs, scratch, mib, flops, args):
    size = sum(a.size * a.dtype.itemsize for a in args)
    return pl.pallas_call(
        kernel,
        out_shape=outs,
        in_specs=ins,
        out_specs=jax.tree.map(lambda _: VMEM, outs),
        scratch_shapes=scratch,
        compiler_params=params(mib),
        cost_estimate=pl.CostEstimate(flops=flops, bytes_accessed=size, transcendentals=0),
    )(*args)


def on_device(residual, gains, w_query, w_key, w_value, w_out, rel_bias):
    tokens = residual.shape[0]
    half = jnp.bfloat16
    place = lax.axis_index(("y", "c")).reshape(1).astype(jnp.int32)
    first = (lax.axis_index("sp") == 0).reshape(1).astype(jnp.int32)
    block = jax.ShapeDtypeStruct((tokens, BLK), half)
    pair = jax.ShapeDtypeStruct((tokens, 2 * BLK), half)
    wide = jax.ShapeDtypeStruct((tokens, BLK), jnp.float32)
    stack = jax.ShapeDtypeStruct((NB, tokens, BLK), half)
    tiles = jax.ShapeDtypeStruct((2, BLK, BLK), jnp.float32)
    flow = lax.axis_size("sp")
    shift = [(i, i + 1) for i in range(flow - 1)]

    def scaled(layer, weights, mib):
        count = len(weights)
        shape = jax.ShapeDtypeStruct((NB, BLK, count * BLK), half)
        scratch = [pltpu.VMEM((D, BLK), half)] * count + [pltpu.SemaphoreType.DMA((count, CUTS))]
        return call(
            functools.partial(scale_kernel, layer, count), [SMEM, VMEM] + [HBM] * count,
            shape, scratch, mib, 10**9, (place, gains, *weights),
        )

    def attention(layer, xs, wq, kv, inv):
        previous = lax.ppermute(kv, "sp", shift)
        local = call(
            functools.partial(local_kernel, layer, len(xs)), [VMEM] * (len(xs) + 4),
            (block, wide, wide, wide, tiles), [], 4, 2 * 10**9, (*xs, wq, inv, kv, rel_bias),
        )
        return call(
            functools.partial(merge_kernel, layer), [SMEM] + [VMEM] * 7, block, [], 4,
            10**9, (first, local[0], previous, *local[1:], rel_bias),
        )

    w_other = lax.ppermute(w_out, "c", [(0, 1), (1, 0)])
    both = jax.ShapeDtypeStruct((2, tokens, BLK), half)
    double = jax.ShapeDtypeStruct((tokens, 2 * BLK), jnp.float32)
    wkv = scaled(0, (w_key, w_value), BIG)
    wq = scaled(0, (w_query,), 4)
    stream = gather_blocks(residual)
    parts = call(
        first_part_kernel, [VMEM] * 3,
        (wide, jax.ShapeDtypeStruct((tokens, 2 * BLK), jnp.float32)), [], 4, 10**9,
        (*stream[:2], wkv),
    )
    kv, inv = call(
        first_kernel, [VMEM] * 4, (pair, wide), [], 4, 10**9, (stream[2], wkv, *parts),
    )
    attended = gather_blocks(attention(0, stream, wq, kv, inv))
    acc = call(
        out_part_kernel, [SMEM] + [VMEM] * 4, double, [], 4, 10**9,
        (place, *attended[:2], w_out, w_other),
    )
    branch = call(
        out_kernel, [SMEM] + [VMEM] * 4, both, [], 4, 10**9,
        (place, attended[2], w_out, w_other, acc),
    )
    branch = gather_blocks(None, branch)
    total = call(squares_kernel, [VMEM] * 2, wide, [], 4, 10**9, branch[:2])
    wkv = scaled(1, (w_key, w_value), 4)
    wq = scaled(1, (w_query,), 4)
    kv, inv, full, carried = call(
        next_kernel, [SMEM] + [VMEM] * 9, (pair, wide, stack, block), [], 4, 2 * 10**9,
        (place, *stream, *branch, total, gains, wkv),
    )
    attended = gather_blocks(attention(1, (full,), wq, kv, inv))
    branch, squares = call(
        last_kernel, [SMEM] + [VMEM] * 4,
        (wide, jax.ShapeDtypeStruct((NB, tokens // BLK, BLK), jnp.float32)), [], 4, 10**9,
        (place, *attended, w_out),
    )
    own_gain = lax.dynamic_slice_in_dim(
        gains[1, 1].reshape(1, D), lax.axis_index(("y", "c")) * BLK, BLK, 1
    )
    everything = lax.all_to_all(squares, ("y", "c"), split_axis=0, concat_axis=0, tiled=True)
    return call(
        finish_kernel, [VMEM] * 4, block, [], 4, 10**7, (everything, branch, carried, own_gain)
    )


def solution(mesh):
    finer = Mesh(mesh.devices.reshape(mesh.shape["sp"], 8, 2), ("sp", "y", "c"))
    tp = ("y", "c")
    in_specs = (
        P("sp", tp),
        P(),
        P(None, None, tp),
        P(None, None, tp),
        P(None, None, tp),
        P(None, None, tp),
        P(None, tp, None),
    )

    return jax.shard_map(
        on_device, mesh=finer, in_specs=in_specs, out_specs=P("sp", tp), check_vma=False
    )
```

```python
import functools

import jax
import jax.numpy as jnp
from jax import lax
from jax.experimental import pallas as pl
from jax.experimental.pallas import tpu as pltpu
from jax.sharding import Mesh
from jax.sharding import PartitionSpec as P


D = 2048
HEAD = 64
BLK = 128
NB = 16
EPS = 1e-06
BIG = 60
CUTS = 8
TILE = 128
NEG = -1e30
VMEM = pl.BlockSpec(memory_space=pltpu.VMEM)
SMEM = pl.BlockSpec(memory_space=pltpu.SMEM)
HBM = pl.BlockSpec(memory_space=pltpu.HBM)


def params(mib):
    return pltpu.CompilerParams(vmem_limit_bytes=mib * 1024 * 1024)


def core_pairs(step):
    pairs = []
    for y in range(8):
        for c in range(2):
            target = (y + (step if c == 0 else -step)) % 8
            pairs.append((2 * y + c, 2 * target + c))
    return pairs


def gather_blocks(x, own=None):
    core = lax.axis_index("c")

    if own is None:
        own = lax.all_gather(x, "c", axis=0)
    two = lax.ppermute(own, ("y", "c"), core_pairs(2))
    one = lax.ppermute(own, ("y", "c"), core_pairs(1))
    half = lax.dynamic_index_in_dim(two, core, 0, keepdims=True)
    three = lax.ppermute(two, ("y", "c"), core_pairs(1))
    four = lax.ppermute(half, ("y", "c"), core_pairs(2))
    received = jnp.concatenate([one, two, three, four], axis=0)
    other = lax.ppermute(received, "c", [(0, 1), (1, 0)])
    return own, received, other


def block_ids(place):
    y, c = place[0] // 2, place[0] % 2
    sign = 1 - 2 * c
    across = 2 * ((y + 4) % 8)
    ids = [2 * y, 2 * y + 1]
    for way, last in ((-sign, c), (sign, 1 - c)):
        for d in (1, 2, 3):
            chip = (y + way * d + 8) % 8
            ids += [2 * chip, 2 * chip + 1]
        ids.append(across + last)
    return ids


def part(refs, k):
    own, received, other = refs
    if k < 2:
        return own, k
    if k < 9:
        return received, k - 2
    return other, k - 9


def scale_kernel(layer, count, place, gain, *refs):
    weights, (out, *held, sems) = refs[:count], refs[count:]
    ids = block_ids(place)
    copies = []
    for n, (w, dst) in enumerate(zip(weights, held)):
        for m in range(CUTS):
            rows = pl.ds(m * (D // CUTS), D // CUTS)
            copies.append(
                pltpu.make_async_copy(w.at[layer, rows, :], dst.at[rows, :], sems.at[n, m])
            )
    for copy in copies:
        copy.start()
    for copy in copies:
        copy.wait()
    for k in range(NB):
        t = ids[k]
        rows = pl.ds(pl.multiple_of(t * BLK, BLK), BLK)
        factor = jnp.broadcast_to(gain_row(gain, layer, 0, t), (BLK, BLK)).T
        for n, w in enumerate(held):
            scaled = w[rows, :].astype(jnp.float32) * factor
            out[k, :, n * BLK : (n + 1) * BLK] = scaled.astype(jnp.bfloat16)


def gain_row(gain, layer, kind, t):
    return gain[layer, kind : kind + 1, pl.ds(pl.multiple_of(t * BLK, BLK), BLK)]


def product(blocks, weights):
    left = jnp.concatenate(blocks, axis=1)
    right = jnp.concatenate(
        [jnp.concatenate([w[k] for w in weights], axis=1) for k in range(len(blocks))], axis=0
    )
    return jnp.dot(left, right, preferred_element_type=jnp.float32)


def blocks_of(refs):
    return [ref[k] for ref in refs for k in range(ref.shape[0])]


def row_squares(refs, rows):
    total = jnp.zeros((rows.size, BLK), jnp.float32)
    for ref in refs:
        for k in range(ref.shape[0]):
            x = ref[k, rows, :].astype(jnp.float32)
            total += x * x
    return total


def tiled(count, body):
    for i in range(count // TILE):
        body(pl.ds(i * TILE, TILE))


def wide_inverse(total):
    inv = lax.rsqrt(jnp.sum(total, axis=1, keepdims=True) / D + EPS)
    return jnp.broadcast_to(inv, total.shape)


def first_part_kernel(own, received, w, total_out, kv_out):
    refs = (own, received)

    def body(rows):
        total_out[rows, :] = row_squares(refs, rows)

    tiled(own.shape[1], body)
    kv_out[...] = product(blocks_of(refs), (w.at[:9],))


def first_kernel(other, w, total, kv_part, kv_out, inv_out):
    def body(rows):
        inv_out[rows, :] = wide_inverse(total[rows, :] + row_squares((other,), rows))

    tiled(other.shape[1], body)
    inv = inv_out[...]
    kv = kv_part[...] + product(blocks_of((other,)), (w.at[9:],))
    kv_out[...] = (kv * jnp.concatenate([inv, inv], axis=1)).astype(jnp.bfloat16)


def squares_kernel(own, received, total_out):
    def body(rows):
        total_out[rows, :] = row_squares((own, received), rows)

    tiled(own.shape[1], body)


def next_kernel(
    place, own, received, other, b_own, b_received, b_other, b_total, gain, w,
    kv_out, inv_out, stream, carried,
):
    ids = block_ids(place)
    mine = place[0] % 2
    refs = (own, received, other)
    b_refs = (b_own, b_received, b_other)

    def body(rows):
        def load(group, k):
            ref, j = part(group, k)
            return ref[j, rows, :].astype(jnp.float32)

        inv_post = wide_inverse(b_total[rows, :] + row_squares((b_other,), rows))
        total = jnp.zeros((TILE, BLK), jnp.float32)
        for k in range(NB):
            x = load(refs, k) + load(b_refs, k) * inv_post * gain_row(gain, 0, 1, ids[k])
            x = x.astype(jnp.bfloat16)
            stream[k, rows, :] = x
            x = x.astype(jnp.float32)
            total += x * x
        inv_out[rows, :] = wide_inverse(total)
        carried[rows, :] = stream[mine, rows, :]

    tiled(own.shape[1], body)
    inv = inv_out[...]
    kv = product(blocks_of((stream,)), (w,))
    kv_out[...] = (kv * jnp.concatenate([inv, inv], axis=1)).astype(jnp.bfloat16)


def grids():
    lane = lax.broadcasted_iota(jnp.int32, (BLK, BLK), 1)
    row = lax.broadcasted_iota(jnp.int32, (BLK, BLK), 0)
    return lane, row


def split_bias(bias, layer, h):
    low = bias[layer, h : h + 1, 0:BLK]
    high = bias[layer, h : h + 1, BLK : 2 * BLK]
    last = bias[layer, h : h + 1, 2 * BLK : 2 * BLK + 1]
    return low, high, last


def skewed(left, right):
    full = jnp.broadcast_to(jnp.concatenate([left, right], axis=1), (BLK, 2 * BLK))
    return pltpu.roll(full, 0, 1, stride=1, stride_axis=0)[:, :BLK].T


def padded_values(kv):
    values = kv[:, BLK:]
    lane = lax.broadcasted_iota(jnp.int32, values.shape, 1)
    one = jnp.ones_like(values)
    return jnp.where(lane < HEAD, values, one), jnp.where(lane < HEAD, one, values)


def head_scores(qh, keys):
    dims = (((1,), (1,)), ((), ()))
    return lax.dot_general(qh, keys, dims, preferred_element_type=jnp.float32)


def local_kernel(layer, x_count, *refs):
    xs, rest = refs[:x_count], refs[x_count:]
    w, inv, kv, bias, q_out, acc_out, top_out, sum_out, near_out = rest
    q = product(blocks_of(xs), (w,))
    q_out[...] = (q * inv[...] * HEAD ** (-0.5)).astype(jnp.bfloat16)
    lane, row = grids()
    values = padded_values(kv)
    tables = []
    for h in range(2):
        low, high, last = split_bias(bias, layer, h)
        last_row = jnp.broadcast_to(last, (1, BLK))
        diag = jnp.where((lane >= 64) & (row < 64), NEG, skewed(high, low))
        near_out[h] = skewed(last_row, high)
        tables.append((diag, near_out[h], jnp.broadcast_to(last, (BLK, BLK))))
    for i in range(4):
        rows = slice(i * BLK, (i + 1) * BLK)
        found = []
        for h in range(2):
            qh = q_out[rows, :]
            qh = jnp.where((lane < HEAD) == (h == 0), qh, jnp.zeros_like(qh))
            raw = head_scores(qh, kv[: (i + 1) * BLK, :BLK])
            scores = [
                raw[:, j * BLK : (j + 1) * BLK] + tables[h][min(i - j, 2)] for j in range(i + 1)
            ]
            top = jnp.max(functools.reduce(jnp.maximum, scores), axis=1, keepdims=True)
            weights = [jnp.exp(s - top).astype(jnp.bfloat16) for s in scores]
            probs = jnp.concatenate(weights, axis=1)
            acc = jnp.dot(probs, values[h][: (i + 1) * BLK], preferred_element_type=jnp.float32)
            found.append((acc, top))
        for n, out in enumerate((acc_out, top_out)):
            out[rows, :] = jnp.where(lane < HEAD, found[0][n], found[1][n])
        sum_out[rows, :] = jnp.where(lane < HEAD, found[1][0], found[0][0])


def merge_kernel(layer, first, q, kv, acc, top, total, nears, bias, out):
    lane, row = grids()
    values = padded_values(kv)
    hidden = jnp.where(first[0] == 1, NEG, 0.0)
    tables = []
    for h in range(2):
        last = split_bias(bias, layer, h)[2]
        full = jnp.broadcast_to(last, (BLK, BLK)) + hidden
        edge = jnp.where((lane < 64) & (row >= 64), NEG, full)
        tables.append((nears[h] + hidden, full, edge))
    where = [(i, h) for i in range(4) for h in range(2)]
    raw, peaks, olds, found = {}, {}, {}, {}
    for i, h in where:
        qh = q[i * BLK : (i + 1) * BLK, :]
        qh = jnp.where((lane < HEAD) == (h == 0), qh, jnp.zeros_like(qh))
        raw[i, h] = head_scores(qh, kv[i * BLK :, :BLK])
    for i, h in where:
        near, full, edge = tables[h]
        scores = []
        for j in range(4 - i):
            term = edge if j == 0 else near if j == 3 else full
            scores.append(raw[i, h][:, j * BLK : (j + 1) * BLK] + term)
        raw[i, h] = scores
        olds[i, h] = top[i * BLK : (i + 1) * BLK, h * HEAD : h * HEAD + 1]
        peak = jnp.max(functools.reduce(jnp.maximum, scores), axis=1, keepdims=True)
        peaks[i, h] = jnp.maximum(peak, olds[i, h])
    for i, h in where:
        weights = [jnp.exp(s - peaks[i, h]).astype(jnp.bfloat16) for s in raw[i, h]]
        probs = jnp.concatenate(weights, axis=1)
        found[i, h] = jnp.dot(probs, values[h][i * BLK :], preferred_element_type=jnp.float32)
    for i in range(4):
        rows = slice(i * BLK, (i + 1) * BLK)
        fades = [jnp.exp(olds[i, h] - peaks[i, h]) for h in range(2)]
        more, fade = (jnp.where(lane < HEAD, x, z) for x, z in ((found[i, 0], found[i, 1]), fades))
        sums = jnp.where(lane < HEAD, found[i, 1], found[i, 0])
        sums_fade = jnp.where(lane < HEAD, fades[1], fades[0])
        norm = pltpu.roll(total[rows, :] * sums_fade + sums, HEAD, 1)
        out[rows, :] = ((acc[rows, :] * fade + more) / norm).astype(jnp.bfloat16)


def rows_product(layer, ids, offset, refs, weights):
    count = sum(ref.shape[0] for ref in refs)
    rows = [
        pl.ds(pl.multiple_of(ids[offset + k] * BLK, BLK), BLK) for k in range(count)
    ]
    right = jnp.concatenate(
        [jnp.concatenate([w[layer, r, :] for w in weights], axis=1) for r in rows], axis=0
    )
    left = jnp.concatenate(blocks_of(refs), axis=1)
    return jnp.dot(left, right, preferred_element_type=jnp.float32)


def out_part_kernel(place, own, received, w, w_other, acc):
    acc[...] = rows_product(0, block_ids(place), 0, (own, received), (w, w_other))


def out_kernel(place, other, w, w_other, acc, out):
    core = place[0] % 2
    total = acc[...] + rows_product(0, block_ids(place), 9, (other,), (w, w_other))
    out[core] = total[:, :BLK].astype(jnp.bfloat16)
    out[1 - core] = total[:, BLK:].astype(jnp.bfloat16)


def last_part_kernel(place, own, received, w, acc):
    acc[...] = rows_product(1, block_ids(place), 0, (own, received), (w,))


def last_kernel(place, other, w, acc, out, squares):
    total = acc[...] + rows_product(1, block_ids(place), 9, (other,), (w,))
    out[...] = total
    for i in range(4):
        x = total[i * BLK : (i + 1) * BLK, :]
        sums = jnp.sum((x * x).T, axis=0, keepdims=True)
        for n in range(NB):
            squares[n, i : i + 1, :] = sums


def finish_kernel(squares, branch, stream, gain, out):
    total = jnp.sum(squares[...], axis=0)
    inv = lax.rsqrt(total / D + EPS)
    for i in range(4):
        rows = slice(i * BLK, (i + 1) * BLK)
        scale = jnp.broadcast_to(inv[i : i + 1, :], (BLK, BLK)).T
        x = stream[rows, :].astype(jnp.float32)
        out[rows, :] = (x + branch[rows, :] * scale * gain[...]).astype(jnp.bfloat16)


def call(kernel, ins, outs, scratch, mib, flops, args):
    size = sum(a.size * a.dtype.itemsize for a in args)
    return pl.pallas_call(
        kernel,
        out_shape=outs,
        in_specs=ins,
        out_specs=jax.tree.map(lambda _: VMEM, outs),
        scratch_shapes=scratch,
        compiler_params=params(mib),
        cost_estimate=pl.CostEstimate(flops=flops, bytes_accessed=size, transcendentals=0),
    )(*args)


def on_device(residual, gains, w_query, w_key, w_value, w_out, rel_bias):
    tokens = residual.shape[0]
    half = jnp.bfloat16
    place = lax.axis_index(("y", "c")).reshape(1).astype(jnp.int32)
    first = (lax.axis_index("sp") == 0).reshape(1).astype(jnp.int32)
    block = jax.ShapeDtypeStruct((tokens, BLK), half)
    pair = jax.ShapeDtypeStruct((tokens, 2 * BLK), half)
    wide = jax.ShapeDtypeStruct((tokens, BLK), jnp.float32)
    stack = jax.ShapeDtypeStruct((NB, tokens, BLK), half)
    tiles = jax.ShapeDtypeStruct((2, BLK, BLK), jnp.float32)
    flow = lax.axis_size("sp")
    shift = [(i, i + 1) for i in range(flow - 1)]

    def scaled(layer, weights, mib):
        count = len(weights)
        shape = jax.ShapeDtypeStruct((NB, BLK, count * BLK), half)
        scratch = [pltpu.VMEM((D, BLK), half)] * count + [pltpu.SemaphoreType.DMA((count, CUTS))]
        return call(
            functools.partial(scale_kernel, layer, count), [SMEM, VMEM] + [HBM] * count,
            shape, scratch, mib, 10**9, (place, gains, *weights),
        )

    def attention(layer, xs, wq, kv, inv):
        previous = lax.ppermute(kv, "sp", shift)
        local = call(
            functools.partial(local_kernel, layer, len(xs)), [VMEM] * (len(xs) + 4),
            (block, wide, wide, wide, tiles), [], 4, 2 * 10**9, (*xs, wq, inv, kv, rel_bias),
        )
        return call(
            functools.partial(merge_kernel, layer), [SMEM] + [VMEM] * 7, block, [], 4,
            10**9, (first, local[0], previous, *local[1:], rel_bias),
        )

    w_other = lax.ppermute(w_out, "c", [(0, 1), (1, 0)])
    both = jax.ShapeDtypeStruct((2, tokens, BLK), half)
    double = jax.ShapeDtypeStruct((tokens, 2 * BLK), jnp.float32)
    wkv = scaled(0, (w_key, w_value), BIG)
    wq = scaled(0, (w_query,), 4)
    stream = gather_blocks(residual)
    parts = call(
        first_part_kernel, [VMEM] * 3,
        (wide, jax.ShapeDtypeStruct((tokens, 2 * BLK), jnp.float32)), [], 4, 10**9,
        (*stream[:2], wkv),
    )
    kv, inv = call(
        first_kernel, [VMEM] * 4, (pair, wide), [], 4, 10**9, (stream[2], wkv, *parts),
    )
    attended = gather_blocks(attention(0, stream, wq, kv, inv))
    acc = call(
        out_part_kernel, [SMEM] + [VMEM] * 4, double, [], 4, 10**9,
        (place, *attended[:2], w_out, w_other),
    )
    branch = call(
        out_kernel, [SMEM] + [VMEM] * 4, both, [], 4, 10**9,
        (place, attended[2], w_out, w_other, acc),
    )
    branch = gather_blocks(None, branch)
    total = call(squares_kernel, [VMEM] * 2, wide, [], 4, 10**9, branch[:2])
    wkv = scaled(1, (w_key, w_value), 4)
    wq = scaled(1, (w_query,), 4)
    kv, inv, full, carried = call(
        next_kernel, [SMEM] + [VMEM] * 9, (pair, wide, stack, block), [], 4, 2 * 10**9,
        (place, *stream, *branch, total, gains, wkv),
    )
    attended = gather_blocks(attention(1, (full,), wq, kv, inv))
    acc = call(
        last_part_kernel, [SMEM] + [VMEM] * 3, wide, [], 4, 10**9,
        (place, *attended[:2], w_out),
    )
    branch, squares = call(
        last_kernel, [SMEM] + [VMEM] * 3,
        (wide, jax.ShapeDtypeStruct((NB, tokens // BLK, BLK), jnp.float32)), [], 4, 10**9,
        (place, attended[2], w_out, acc),
    )
    own_gain = lax.dynamic_slice_in_dim(
        gains[1, 1].reshape(1, D), lax.axis_index(("y", "c")) * BLK, BLK, 1
    )
    everything = lax.all_to_all(squares, ("y", "c"), split_axis=0, concat_axis=0, tiled=True)
    return call(
        finish_kernel, [VMEM] * 4, block, [], 4, 10**7, (everything, branch, carried, own_gain)
    )


def solution(mesh):
    finer = Mesh(mesh.devices.reshape(mesh.shape["sp"], 8, 2), ("sp", "y", "c"))
    tp = ("y", "c")
    in_specs = (
        P("sp", tp),
        P(),
        P(None, None, tp),
        P(None, None, tp),
        P(None, None, tp),
        P(None, None, tp),
        P(None, tp, None),
    )

    return jax.shard_map(
        on_device, mesh=finer, in_specs=in_specs, out_specs=P("sp", tp), check_vma=False
    )
```
